128 devices in a mesh: sp: 16 (over z, x), dp: 8 (over y, core).
Axes of the slice: x: 4, y: 4, z: 4, core: 2. Of those that a mesh axis runs over, the one named last changes fastest.
Arguments:
- hidden_in: bfloat16 [8, 2048, 2048], P('dp', 'sp'), may hold values from -6 to 6
- mix_cotangent: bfloat16 [8, 2048, 4096], P('dp', 'sp'), may hold values from -0.119628906 to 0.119628906
- query_weight: bfloat16 [2048, 4096], P('dp', 'sp'), may hold values from -0.125 to 0.125
- key_weight: bfloat16 [2048, 4096], P('dp', 'sp'), may hold values from -0.125 to 0.125
- value_weight: bfloat16 [2048, 4096], P('dp', 'sp'), may hold values from -0.125 to 0.125
- decay_log: float32 [16], P('sp'), may hold values from -0.034 to -0.000146484375, as said below
Outputs:
- grad_hidden: bfloat16 [8, 2048, 2048], P('dp', 'sp')
- grad_query: float32 [2048, 4096], P('dp', 'sp')
- grad_key: float32 [2048, 4096], P('dp', 'sp')
- grad_value: float32 [2048, 4096], P('dp', 'sp')
The draws below stay inside these ranges and needn't reach their ends.
Inputs may be any that keep to these rules, and one draw needn't show every extreme that they name: Each head's decay_log is negative.
All inputs are finite; a program needn't handle non-finite values.
Results may differ from the reference program's by a relative error of at most 0.015.
Values may be sent and summed in bfloat16 or wider, within the bound.
A program may use at most 64 MiB of HBM per device.

```python
import jax
import jax.numpy as jnp
from jax import lax

D = 2048
HEADS = 16
BLOCK = 128
WIDTH = 4096
SEQ_LEN = 2048
SEQS = 8
N_SP = 16


def draw_decay_log(key, part):
    key_fast = jax.random.fold_in(key, 11)
    key_quick = jax.random.fold_in(key, 12)
    key_slow = jax.random.fold_in(key, 13)
    fast = jax.random.bernoulli(key_fast, 0.5, (HEADS,))
    quick_rate = jax.random.uniform(key_quick, (HEADS,), jnp.float32, 0.01, 0.034)
    slow_rate = jax.random.uniform(key_slow, (HEADS,), jnp.float32, 0.3, 2.0) / SEQ_LEN
    return -jnp.where(fast, quick_rate, slow_rate).astype(jnp.float32)


def block_levels(own_key, extent, cuts, smallest, largest):
    gain = 1.0
    for position, parts in cuts:
        heights = jax.random.uniform(jax.random.fold_in(jax.random.fold_in(own_key, 6), position), (parts,), jnp.float32, smallest / len(cuts), largest / len(cuts))
        gain = gain * jnp.repeat(jnp.exp(heights), extent[position] // parts).reshape((-1,) + (1,) * (len(extent) - 1 - position))
    return gain


def noise(rng, extent, scale, reach, split=(), kind=jnp.bfloat16):
    array = scale * jax.random.normal(rng, extent, jnp.float32)
    if split:
        array = array * block_levels(rng, extent, split, -0.22, 0.18)
    return jnp.clip(array, -reach, reach).astype(kind)


def setup_inputs(seed: int = 0) -> dict:
    seeds = jax.random.split(jax.random.key(seed), 7)
    return {
        "hidden_in": noise(seeds[0], (SEQS, SEQ_LEN, D), 1.0, 6.0, ((0, 8), (1, 16))),
        "mix_cotangent": noise(seeds[1], (SEQS, SEQ_LEN, WIDTH), 0.02, 0.119628906, ((0, 8), (1, 16))),
        "query_weight": noise(seeds[2], (D, WIDTH), D ** -0.5, 0.125, ((0, 8), (1, 16))),
        "key_weight": noise(seeds[3], (D, WIDTH), D ** -0.5, 0.125, ((0, 8), (1, 16))),
        "value_weight": noise(seeds[4], (D, WIDTH), D ** -0.5, 0.125, ((0, 8), (1, 16))),
        "decay_log": draw_decay_log(jax.random.fold_in(seeds[6], 71), 0),
    }


def head_grads(queries, key_rows, values, cotangent, log_rate):
    length = queries.shape[0]
    head_dim = queries.shape[1]
    blocks = length // BLOCK
    scale = head_dim ** -0.5
    keys_scaled = (key_rows.astype(jnp.float32) * scale).astype(jnp.bfloat16)
    offsets = jnp.arange(BLOCK, dtype=jnp.float32)
    spread = offsets[:, None] - offsets[None, :]
    inner_decay = jnp.where(spread >= 0, jnp.exp(log_rate * jnp.maximum(spread, 0.0)), 0.0)
    query_decay = jnp.exp(log_rate * (offsets + 1.0))
    key_decay = jnp.exp(log_rate * (BLOCK - 1.0 - offsets))
    block_decay = jnp.exp(log_rate * BLOCK)

    def split_blocks(series):
        return series.reshape(blocks, BLOCK, series.shape[-1])

    def forward(carried, inputs):
        query_block, key_block, value_block, grad_block = inputs
        mixed = (jnp.dot(grad_block, value_block.T, preferred_element_type=jnp.float32) * inner_decay).astype(jnp.bfloat16)
        within = jnp.dot(mixed, key_block, preferred_element_type=jnp.float32)
        across = jnp.dot(grad_block, carried.astype(jnp.bfloat16).T, preferred_element_type=jnp.float32) * query_decay[:, None]
        weighted = (key_block.astype(jnp.float32) * key_decay[:, None]).astype(jnp.bfloat16)
        updated = carried * block_decay + jnp.dot(weighted.T, value_block, preferred_element_type=jnp.float32)
        return updated, (within + across, mixed)

    def backward(carried, inputs):
        query_block, key_block, value_block, grad_block, mixed = inputs
        scores = (jnp.dot(query_block, key_block.T, preferred_element_type=jnp.float32) * inner_decay).astype(jnp.bfloat16)
        state_bf = carried.astype(jnp.bfloat16)
        grad_v = jnp.dot(scores.T, grad_block, preferred_element_type=jnp.float32) + jnp.dot(key_block, state_bf, preferred_element_type=jnp.float32) * key_decay[:, None]
        grad_k = (jnp.dot(mixed.T, query_block, preferred_element_type=jnp.float32) + jnp.dot(value_block, state_bf.T, preferred_element_type=jnp.float32) * key_decay[:, None]) * scale
        weighted = (query_block.astype(jnp.float32) * query_decay[:, None]).astype(jnp.bfloat16)
        updated = carried * block_decay + jnp.dot(weighted.T, grad_block, preferred_element_type=jnp.float32)
        return updated, (grad_k, grad_v)

    inputs = (split_blocks(queries), split_blocks(keys_scaled), split_blocks(values), split_blocks(cotangent))
    initial = jnp.zeros((head_dim, values.shape[-1]), jnp.float32)
    final_state, (grad_q, mixed_all) = lax.scan(forward, initial, inputs)
    final_back, (grad_k, grad_v) = lax.scan(backward, initial, inputs + (mixed_all,), reverse=True)
    return grad_q.reshape(length, -1), grad_k.reshape(length, -1), grad_v.reshape(length, -1)


def group_grads(log_rates, queries, key_rows, values, cotangent):
    length = queries.shape[0]
    head_count = log_rates.shape[0]

    def by_head(series):
        return series.reshape(length, head_count, -1).transpose(1, 0, 2)

    def to_rows(series):
        return series.transpose(1, 0, 2).reshape(length, -1)

    grad_q, grad_k, grad_v = jax.vmap(head_grads)(by_head(queries), by_head(key_rows), by_head(values), by_head(cotangent), log_rates)
    return jnp.concatenate((to_rows(grad_q), to_rows(grad_k), to_rows(grad_v)), axis=1).astype(jnp.bfloat16)


def reference(hidden_in, mix_cotangent, query_weight, key_weight, value_weight, decay_log):
    weights = jnp.concatenate((query_weight, key_weight, value_weight), axis=1)
    all_width = query_weight.shape[1]
    model_width = query_weight.shape[0]

    def one_sequence(seq_pair):
        seq_rows, seq_cotangent = seq_pair
        projected = jnp.dot(seq_rows, weights, preferred_element_type=jnp.float32).astype(jnp.bfloat16)
        gradients = group_grads(decay_log, projected[:, :all_width], projected[:, all_width:2 * all_width], projected[:, 2 * all_width:], seq_cotangent)
        length = seq_rows.shape[0]
        split_grads = gradients.reshape(length, 3, N_SP, -1).astype(jnp.float32)
        split_weights = weights.reshape(model_width, 3, N_SP, -1).astype(jnp.float32)
        partials = jnp.einsum('ltgc,dtgc->gld', split_grads, split_weights)
        rounded = lax.optimization_barrier(partials.astype(jnp.bfloat16)).astype(jnp.float32)
        return jnp.sum(rounded, axis=0).astype(jnp.bfloat16), gradients

    grad_hidden, all_grads = lax.map(one_sequence, (hidden_in, mix_cotangent))
    flat_rows = hidden_in.reshape(-1, model_width)
    flat_grads = all_grads.reshape(-1, 3 * all_width)
    summed = lax.dot_general(flat_rows, flat_grads, (((0,), (0,)), ((), ())), preferred_element_type=jnp.float32) / SEQS
    return grad_hidden, summed[:, :all_width], summed[:, all_width:2 * all_width], summed[:, 2 * all_width:]
```

```python
import functools

import jax
import jax.numpy as jnp
from jax import lax
from jax.experimental import pallas as pl
from jax.experimental.pallas import tpu as pltpu
from jax.sharding import PartitionSpec as P

BLOCK = 128
F32 = jnp.float32
BF16 = jnp.bfloat16


def dot(a, b):
    return lax.dot_general(a, b, (((1,), (0,)), ((), ())), preferred_element_type=F32)


def dot_t(a, b):
    return lax.dot_general(a, b, (((1,), (1,)), ((), ())), preferred_element_type=F32)


def t_dot(a, b):
    return lax.dot_general(a, b, (((0,), (0,)), ((), ())), preferred_element_type=F32)


def rows_of(block):
    return pl.ds(pl.multiple_of(block * BLOCK, BLOCK), BLOCK)


def make_decays(rate, inner_ref, inner_t_ref, query_ref, key_ref):
    row = lax.broadcasted_iota(jnp.int32, (BLOCK, BLOCK), 0)
    col = lax.broadcasted_iota(jnp.int32, (BLOCK, BLOCK), 1)
    spread = (row - col).astype(F32)
    inner_ref[...] = jnp.where(spread >= 0, jnp.exp(rate * jnp.maximum(spread, 0.0)), 0.0)
    inner_t_ref[...] = jnp.where(spread <= 0, jnp.exp(rate * jnp.maximum(-spread, 0.0)), 0.0)
    offset = lax.broadcasted_iota(jnp.int32, query_ref.shape, 0).astype(F32)
    query_ref[...] = jnp.exp(rate * (offset + 1.0))
    key_ref[...] = jnp.exp(rate * (BLOCK - 1.0 - offset))


def in_block(block, head, scale, qkv, cot, decays, grads, fwd_states, bwd_states):
    inner_ref, inner_t_ref, query_ref, key_ref = decays
    rows = rows_of(block)
    queries = qkv[rows, 0:head]
    keys = qkv[rows, head : 2 * head]
    values = qkv[rows, 2 * head : 3 * head]
    given = cot[rows, :]
    mixed = (dot_t(given, values) * inner_ref[...]).astype(BF16)
    grads[rows, 0:head] = dot(mixed, keys)
    mixed_t = (dot_t(values, given) * inner_t_ref[...]).astype(BF16)
    grads[rows, head : 2 * head] = dot(mixed_t, queries) * scale
    scores_t = (dot_t(keys, queries) * inner_t_ref[...]).astype(BF16)
    grads[rows, 2 * head : 3 * head] = dot(scores_t, given)
    keys_w = (keys.astype(F32) * key_ref[...]).astype(BF16)
    fwd_states[block] = t_dot(keys_w, values)
    queries_w = (queries.astype(F32) * query_ref[...]).astype(BF16)
    bwd_states[block] = t_dot(queries_w, given)


def run_states(rate, blocks, fwd_states, bwd_states, fwd_bf, bwd_bf):
    step = jnp.exp(jnp.full(fwd_states.shape[1:], BLOCK, F32) * rate)

    def forward(i, carried):
        fwd_bf[i] = carried.astype(BF16)
        return carried * step + fwd_states[i]

    lax.fori_loop(0, blocks, forward, jnp.zeros(fwd_states.shape[1:], F32))

    def backward(n, carried):
        i = blocks - 1 - n
        bwd_bf[i] = carried.astype(BF16)
        return carried * step + bwd_states[i]

    lax.fori_loop(0, blocks, backward, jnp.zeros(fwd_states.shape[1:], F32))


def cross_block(block, head, scale, qkv, cot, decays, grads, fwd_bf, bwd_bf, out):
    _, _, query_ref, key_ref = decays
    rows = rows_of(block)
    keys = qkv[rows, head : 2 * head]
    values = qkv[rows, 2 * head : 3 * head]
    state = fwd_bf[block]
    back = bwd_bf[block]
    grad_q = grads[rows, 0:head] + dot_t(cot[rows, :], state) * query_ref[...]
    grad_k = grads[rows, head : 2 * head] + dot_t(values, back) * (key_ref[...] * scale)
    grad_v = grads[rows, 2 * head : 3 * head] + dot(keys, back) * key_ref[...]
    out[rows, 0:head] = grad_q.astype(BF16)
    out[rows, head : 2 * head] = grad_k.astype(BF16)
    out[rows, 2 * head : 3 * head] = grad_v.astype(BF16)


def mixer_kernel(rate_ref, rows_ref, weight_ref, cot_ref, out_ref, qkv, grads, inner, inner_t, query_d, key_d, fwd, bwd, fwd_bf, bwd_bf):
    length, wide = out_ref.shape
    head = wide // 3
    blocks = length // BLOCK
    scale = head ** (-0.5)
    rate = rate_ref[0]
    decays = (inner, inner_t, query_d, key_d)
    make_decays(rate, *decays)

    def project(n, _):
        rows = rows_of(n)
        got = dot(rows_ref[rows, :], weight_ref[...])
        qkv[rows, 0:head] = got[:, 0:head].astype(BF16)
        qkv[rows, head : 2 * head] = (got[:, head : 2 * head].astype(BF16).astype(F32) * scale).astype(BF16)
        qkv[rows, 2 * head : 3 * head] = got[:, 2 * head : 3 * head].astype(BF16)
        return _

    lax.fori_loop(0, blocks, project, 0)

    def inside(n, _):
        in_block(n, head, scale, qkv, cot_ref, decays, grads, fwd, bwd)
        return _

    lax.fori_loop(0, blocks, inside, 0)
    run_states(rate, blocks, fwd, bwd, fwd_bf, bwd_bf)

    def across(n, _):
        cross_block(n, head, scale, qkv, cot_ref, decays, grads, fwd_bf, bwd_bf, out_ref)
        return _

    lax.fori_loop(0, blocks, across, 0)


def mixer(rate, rows, weights, cot):
    length = rows.shape[0]
    wide = weights.shape[1]
    head = wide // 3
    blocks = length // BLOCK
    vmem = pl.BlockSpec(memory_space=pltpu.VMEM)
    return pl.pallas_call(
        mixer_kernel,
        out_shape=jax.ShapeDtypeStruct((length, wide), BF16),
        in_specs=[pl.BlockSpec(memory_space=pltpu.SMEM), vmem, vmem, vmem],
        out_specs=vmem,
        scratch_shapes=[
            pltpu.VMEM((length, wide), BF16),
            pltpu.VMEM((length, wide), F32),
            pltpu.VMEM((BLOCK, BLOCK), F32),
            pltpu.VMEM((BLOCK, BLOCK), F32),
            pltpu.VMEM((BLOCK, head), F32),
            pltpu.VMEM((BLOCK, head), F32),
            pltpu.VMEM((blocks, head, head), F32),
            pltpu.VMEM((blocks, head, head), F32),
            pltpu.VMEM((blocks, head, head), BF16),
            pltpu.VMEM((blocks, head, head), BF16),
        ],
        compiler_params=pltpu.CompilerParams(vmem_limit_bytes=56 * 1024 * 1024),
        cost_estimate=pl.CostEstimate(flops=9 * 10**9, bytes_accessed=20 * 10**6, transcendentals=0),
    )(rate, rows, weights, cot)


def in_blocks(array, dim, size):
    shape = array.shape
    pieces = array.reshape(*shape[:dim], size, shape[dim] // size, *shape[dim + 1 :])
    return jnp.moveaxis(pieces, dim, 0)


def sent_and_summed(array, axis, dim):
    pieces = in_blocks(array, dim, lax.axis_size(axis))
    arrived = lax.all_to_all(pieces, axis, split_axis=0, concat_axis=0, tiled=True)
    return arrived.astype(F32).sum(axis=0)


def body(hidden_in, mix_cotangent, query_weight, key_weight, value_weight, decay_log):
    own_rows = hidden_in[0]
    columns = query_weight.shape[1]
    stacked = jnp.concatenate((query_weight, key_weight, value_weight), axis=1)
    weights = lax.all_gather(stacked, "dp", axis=0, tiled=True)
    cotangent = lax.all_to_all(mix_cotangent[0], "sp", split_axis=1, concat_axis=0, tiled=True)
    all_rows = lax.all_gather(own_rows, "sp", axis=0, tiled=True)
    gradients = mixer(decay_log, all_rows, weights, cotangent)
    input_sum = lax.psum_scatter(
        lax.dot_general(gradients, weights, (((1,), (1,)), ((), ())), preferred_element_type=F32).astype(BF16),
        "sp",
        scatter_dimension=0,
        tiled=True,
    )
    summed = sent_and_summed(
        lax.dot_general(all_rows, gradients, (((0,), (0,)), ((), ())), preferred_element_type=F32).astype(BF16), "dp", 0
    ) / lax.axis_size("dp")
    return (input_sum[None], summed[:, :columns], summed[:, columns : 2 * columns], summed[:, 2 * columns :])


def solution(mesh):
    placed = (P("dp", "sp", None), P("dp", "sp", None), P("dp", "sp"), P("dp", "sp"), P("dp", "sp"), P("sp"))
    return jax.shard_map(
        body,
        mesh=mesh,
        in_specs=placed,
        out_specs=(P("dp", "sp", None), P("dp", "sp"), P("dp", "sp"), P("dp", "sp")),
        check_vma=False,
    )
```

```python
import jax
import jax.numpy as jnp
from jax import lax
from jax.experimental import pallas as pl
from jax.experimental.pallas import tpu as pltpu
from jax.sharding import PartitionSpec as P

BLOCK = 128
HALF = 64
PART = 32
RING = 4
F32 = jnp.float32
BF16 = jnp.bfloat16
MESH = pl.DeviceIdType.MESH
SIDES = (1, -1)


def dot(a, b):
    return lax.dot_general(a, b, (((1,), (0,)), ((), ())), preferred_element_type=F32)


def dot_t(a, b):
    return lax.dot_general(a, b, (((1,), (1,)), ((), ())), preferred_element_type=F32)


def t_dot(a, b):
    return lax.dot_general(a, b, (((0,), (0,)), ((), ())), preferred_element_type=F32)


def rows_of(block):
    return pl.ds(pl.multiple_of(block * BLOCK, BLOCK), BLOCK)


def pick(index, values):
    got = jnp.int32(values[-1])
    for place, value in enumerate(values[:-1]):
        got = jnp.where(index == place, jnp.int32(value), got)
    return got


def add_into(target, rows, others):
    total = target[rows, :].astype(F32)
    for other in others:
        total = total + other.astype(F32)
    target[rows, :] = total.astype(BF16)


def make_decays(rate, inner_ref, inner_t_ref, query_ref, key_ref):
    row = lax.broadcasted_iota(jnp.int32, (BLOCK, BLOCK), 0)
    col = lax.broadcasted_iota(jnp.int32, (BLOCK, BLOCK), 1)
    spread = (row - col).astype(F32)
    inner_ref[...] = jnp.where(spread >= 0, jnp.exp(rate * jnp.maximum(spread, 0.0)), 0.0)
    inner_t_ref[...] = jnp.where(spread <= 0, jnp.exp(rate * jnp.maximum(-spread, 0.0)), 0.0)
    offset = lax.broadcasted_iota(jnp.int32, query_ref.shape, 0).astype(F32)
    query_ref[...] = jnp.exp(rate * (offset + 1.0))
    key_ref[...] = jnp.exp(rate * (BLOCK - 1.0 - offset))


def in_block(block, head, scale, qkv, cot, decays, grads, fwd_states, bwd_states):
    inner_ref, inner_t_ref, query_ref, key_ref = decays
    rows = rows_of(block)
    queries = qkv[rows, 0:head]
    keys = qkv[rows, head : 2 * head]
    values = qkv[rows, 2 * head : 3 * head]
    given = cot[rows, :]
    mixed = (dot_t(given, values) * inner_ref[...]).astype(BF16)
    grads[rows, 0:head] = dot(mixed, keys)
    mixed_t = (dot_t(values, given) * inner_t_ref[...]).astype(BF16)
    grads[rows, head : 2 * head] = dot(mixed_t, queries) * scale
    scores_t = (dot_t(keys, queries) * inner_t_ref[...]).astype(BF16)
    grads[rows, 2 * head : 3 * head] = dot(scores_t, given)
    keys_w = (keys.astype(F32) * key_ref[...]).astype(BF16)
    fwd_states[block] = t_dot(keys_w, values)
    queries_w = (queries.astype(F32) * query_ref[...]).astype(BF16)
    bwd_states[block] = t_dot(queries_w, given)


def run_states(rate, blocks, fwd_states, bwd_states, fwd_bf, bwd_bf):
    step = jnp.exp(jnp.full(fwd_states.shape[1:], BLOCK, F32) * rate)

    def forward(i, carried):
        fwd_bf[i] = carried.astype(BF16)
        return carried * step + fwd_states[i]

    lax.fori_loop(0, blocks, forward, jnp.zeros(fwd_states.shape[1:], F32))

    def backward(n, carried):
        i = blocks - 1 - n
        bwd_bf[i] = carried.astype(BF16)
        return carried * step + bwd_states[i]

    lax.fori_loop(0, blocks, backward, jnp.zeros(fwd_states.shape[1:], F32))


def cross_block(block, head, scale, qkv, cot, decays, grads, fwd_bf, bwd_bf, out):
    _, _, query_ref, key_ref = decays
    rows = rows_of(block)
    keys = qkv[rows, head : 2 * head]
    values = qkv[rows, 2 * head : 3 * head]
    state = fwd_bf[block]
    back = bwd_bf[block]
    grad_q = grads[rows, 0:head] + dot_t(cot[rows, :], state) * query_ref[...]
    grad_k = grads[rows, head : 2 * head] + dot_t(values, back) * (key_ref[...] * scale)
    grad_v = grads[rows, 2 * head : 3 * head] + dot(keys, back) * key_ref[...]
    out[rows, 0:head] = grad_q.astype(BF16)
    out[rows, head : 2 * head] = grad_k.astype(BF16)
    out[rows, 2 * head : 3 * head] = grad_v.astype(BF16)


def all_kernel(
    rate_ref,
    own_x,
    own_cot,
    wq_ref,
    wk_ref,
    wv_ref,
    out_x,
    out_q,
    out_k,
    out_v,
    xall,
    w,
    qkv,
    cot,
    grads,
    inner,
    inner_t,
    query_d,
    key_d,
    fwd,
    bwd,
    fwd_bf,
    bwd_bf,
    g,
    part,
    first1,
    first2,
    second1,
    second2,
    wg,
    pair1,
    ring1,
    ring2,
    local_sem,
    send_sem,
    recv_sem,
):
    depth = xall.shape[1]
    head = cot.shape[1]
    blocks = RING * RING
    scale = head ** (-0.5)
    sp = lax.axis_index("sp")
    dp = lax.axis_index("dp")
    z, x = lax.div(sp, RING), lax.rem(sp, RING)
    y, core = lax.div(dp, 2), lax.rem(dp, 2)
    rate = rate_ref[0]
    decays = (inner, inner_t, query_d, key_d)
    names = {}
    sent = []

    def slot(*name):
        return names.setdefault(name, len(names))

    def wrap(value):
        return lax.rem(value + RING, RING)

    def block_at(dz, dx):
        return wrap(z + dz) * RING + wrap(x + dx)

    def plane(dz, dx):
        return (block_at(dz, dx), dp)

    def along_y(dy):
        return (sp, wrap(y + dy) * 2 + core)

    partner = (sp, y * 2 + 1 - core)

    def along(half, first, second):
        return (second, first) if half == 0 else (first, second)

    def copy(index, source, target, device):
        return pltpu.make_async_remote_copy(
            src_ref=source,
            dst_ref=target,
            send_sem=send_sem.at[index],
            recv_sem=recv_sem.at[index],
            device_id=device,
            device_id_type=MESH,
        )

    def send(index, source, target, device):
        copy(index, source, target, device).start()
        sent.append((index, source))

    def arrived(index, target):
        copy(index, target, target, partner).wait_recv()

    barrier = pltpu.get_barrier_semaphore()
    friends = [plane(dz, dx) for dz in range(RING) for dx in range(RING) if dz or dx]
    friends = friends + [along_y(1), along_y(-1), partner]
    for friend in friends:
        pl.semaphore_signal(barrier, inc=1, device_id=friend, device_id_type=MESH)

    own_rows = rows_of(sp)
    w_rows = pl.ds(pl.multiple_of(dp * head, head), head)
    loads = [
        pltpu.make_async_copy(own_x.at[0], xall.at[own_rows, :], local_sem.at[0]),
        pltpu.make_async_copy(wq_ref, w.at[w_rows, 0:head], local_sem.at[1]),
        pltpu.make_async_copy(wk_ref, w.at[w_rows, head : 2 * head], local_sem.at[2]),
        pltpu.make_async_copy(wv_ref, w.at[w_rows, 2 * head : 3 * head], local_sem.at[3]),
        pltpu.make_async_copy(
            own_cot.at[0, :, pl.ds(pl.multiple_of(sp * head, head), head)], cot.at[own_rows, :], local_sem.at[4]
        ),
    ]
    for load in loads:
        load.start()
    make_decays(rate, *decays)
    for load in loads:
        load.wait()
    pl.semaphore_wait(barrier, len(friends))

    def x_rows(block, start, count):
        return xall.at[pl.ds(pl.multiple_of(block * BLOCK + start, PART), count), :]

    def part_start(half, side):
        return half * HALF + (0 if side == 1 else PART)

    def gather_block(half, p, q):
        return block_at(*along(half, p, q))

    def gather_send(name, half, p, q, side, axis):
        block = gather_block(half, p, q)
        if name[0] in ("s1", "s2"):
            rows = x_rows(block, half * HALF, HALF)
        else:
            rows = x_rows(block, part_start(half, side), PART)
        device = plane(*along(half, side, 0)) if axis == 0 else plane(*along(half, 0, side))
        send(slot(*name), rows, rows, device)

    def gather_wait(name, half, p, q, side):
        block = gather_block(half, p, q)
        if name[0] in ("s1", "s2"):
            rows = x_rows(block, half * HALF, HALF)
        else:
            rows = x_rows(block, part_start(half, side), PART)
        arrived(slot(*name), rows)

    def w_part(dy, which, start, count):
        first = (wrap(y + dy) * 2 + which) * head
        return w.at[pl.ds(pl.multiple_of(first + start, BLOCK), count), :]

    for half in range(2):
        for side in SIDES:
            gather_send(("s1", half, side), half, 0, 0, side, 0)
    for side in SIDES:
        send(slot("w1", side), w_part(0, core, 0, head), w_part(0, core, 0, head), along_y(side))
    send(slot("wc", 0), w_part(0, core, 0, head), w_part(0, core, 0, head), partner)
    for half in range(2):
        for side in SIDES:
            gather_send(("s2", half, 0, side), half, 0, 0, side, 1)
    for offset in A2A_ORDER:
        target = lax.rem(sp + offset, blocks)
        send(
            slot("cot", offset),
            own_cot.at[0, :, pl.ds(pl.multiple_of(target * head, head), head)],
            cot.at[own_rows, :],
            (target, dp),
        )

    def project(block):
        rows = rows_of(block)
        got = dot(xall[rows, :], w[...])
        qkv[rows, 0:head] = got[:, 0:head].astype(BF16)
        qkv[rows, head : 2 * head] = (got[:, head : 2 * head].astype(BF16).astype(F32) * scale).astype(BF16)
        qkv[rows, 2 * head : 3 * head] = got[:, 2 * head : 3 * head].astype(BF16)

    def inside(block):
        in_block(block, head, scale, qkv, cot, decays, grads, fwd, bwd)

    def loop(places, *works):
        def step(n, carried):
            block = block_at(pick(n, [dz for dz, _ in places]), pick(n, [dx for _, dx in places]))
            for work in works:
                work(block)
            return carried

        lax.fori_loop(0, len(places), step, 0)

    near = [(0, 0), (0, 1), (0, 3), (1, 0), (3, 0)]
    corners = [(1, 1), (1, 3), (3, 1), (3, 3)]
    far = [(0, 2), (2, 0)]
    edges = [(1, 2), (3, 2), (2, 1), (2, 3)]
    last = [(2, 2)]

    for half in range(2):
        for side in SIDES:
            gather_wait(("s1", half, side), half, -side, 0, side)
            gather_send(("f1", half, side), half, -side, 0, side, 0)
    for half in range(2):
        for near_p in SIDES:
            for side in SIDES:
                gather_send(("s2", half, near_p, side), half, near_p, 0, side, 1)

    for side in SIDES:
        arrived(slot("w1", side), w_part(-side, core, 0, head))
        rows = w_part(-side, core, 0 if side == 1 else BLOCK, BLOCK)
        send(slot("w2", side), rows, rows, along_y(side))
        rows = w_part(-side, core, 0, head)
        send(slot("wc", side), rows, rows, partner)

    for half in range(2):
        for side in SIDES:
            gather_wait(("s2", half, 0, side), half, 0, -side, side)
            gather_send(("f2", half, 0, side), half, 0, -side, side, 1)

    for side in SIDES:
        arrived(slot("w2", side), w_part(2, core, 0 if side == 1 else BLOCK, BLOCK))
    send(slot("wc", 2), w_part(2, core, 0, head), w_part(2, core, 0, head), partner)
    for dy in (0, 1, -1, 2):
        arrived(slot("wc", dy), w_part(-dy, 1 - core, 0, head))

    loop(near, project)

    for half in range(2):
        for side in SIDES:
            gather_wait(("f1", half, side), half, 2, 0, side)
    for half in range(2):
        for side in SIDES:
            gather_send(("s2", half, 2, side), half, 2, 0, side, 1)

    for offset in A2A_ORDER:
        arrived(slot("cot", offset), cot.at[rows_of(lax.rem(sp + blocks - offset, blocks)), :])
    loop(near, inside)

    for near_p in SIDES:
        for half in range(2):
            for side in SIDES:
                gather_wait(("s2", half, near_p, side), half, near_p, -side, side)
                gather_send(("f2", half, near_p, side), half, near_p, -side, side, 1)
    loop(corners, project, inside)

    for half in range(2):
        for side in SIDES:
            gather_wait(("f2", half, 0, side), half, 0, 2, side)
    loop(far, project, inside)

    for half in range(2):
        for side in SIDES:
            gather_wait(("s2", half, 2, side), half, 2, -side, side)
            gather_send(("f2", half, 2, side), half, 2, -side, side, 1)

    for near_p in SIDES:
        for half in range(2):
            for side in SIDES:
                gather_wait(("f2", half, near_p, side), half, near_p, 2, side)
    loop(edges, project, inside)

    for half in range(2):
        for side in SIDES:
            gather_wait(("f2", half, 2, side), half, 2, 2, side)
    loop(last, project, inside)

    run_states(rate, blocks, fwd, bwd, fwd_bf, bwd_bf)

    def finish(block):
        cross_block(block, head, scale, qkv, cot, decays, grads, fwd_bf, bwd_bf, g)
        rows = rows_of(block)
        part[rows, :] = dot_t(g[rows, :], w[...]).astype(BF16)

    def sum_block(half, f, q):
        return block_at(*((f, q) if half == 0 else (q, f)))

    def sum_rows(block, start, count):
        return pl.ds(pl.multiple_of(block * BLOCK + start, PART), count)

    def f_device(half, side):
        return plane(side, 0) if half == 0 else plane(0, side)

    def g_device(half, side):
        return plane(0, side) if half == 0 else plane(side, 0)

    def which(side):
        return 0 if side == 1 else 1

    def send_first(half, j):
        for side in SIDES:
            rows = sum_rows(sum_block(half, 2, j), part_start(half, side), PART)
            send(slot("F1", half, j, side), part.at[rows, :], first1.at[half, which(side), j], f_device(half, side))

    def send_second(half, j):
        for side in SIDES:
            block = sum_block(half, side, j)
            rows = sum_rows(block, part_start(half, side), PART)
            arrived(slot("F1", half, j, side), first1.at[half, which(side), j])
            add_into(part, rows, [first1[half, which(side), j]])
        for side in SIDES:
            block = sum_block(half, side, j)
            rows = sum_rows(block, half * HALF, HALF)
            send(slot("F2", half, j, side), part.at[rows, :], first2.at[half, which(side), j], f_device(half, side))

    def take_second(half, j):
        for side in SIDES:
            arrived(slot("F2", half, j, side), first2.at[half, which(side), j])
        rows = sum_rows(sum_block(half, 0, j), half * HALF, HALF)
        add_into(part, rows, [first2[half, 0, j], first2[half, 1, j]])

    loop([(2, 2), (2, 1), (2, 3), (2, 0)], finish)
    for j in (2, 1, 3, 0):
        send_first(0, j)
    send_first(1, 2)
    loop([(1, 2), (3, 2), (0, 2)], finish)
    for j in (1, 3, 0):
        send_first(1, j)
    loop(corners, finish)
    for half in range(2):
        send_second(half, 2)
    loop([(1, 0), (3, 0), (0, 1), (0, 3), (0, 0)], finish)
    for j in (1, 3, 0):
        for half in range(2):
            send_second(half, j)

    def weight_part(chunk):
        columns = pl.ds(pl.multiple_of(chunk * head, head), head)
        wg[chunk] = t_dot(xall[:, columns], g[...]).astype(BF16)

    ahead = (2, 1, 3, 0)

    def others(n, carried):
        weight_part(wrap(y + pick(n, ahead)) * 2 + 1 - core)
        return carried

    lax.fori_loop(0, RING, others, 0)
    for n in range(RING):
        chunk = wrap(y + ahead[n]) * 2 + 1 - core
        send(slot("pair", n), wg.at[chunk], pair1.at[n], partner)

    for half in range(2):
        take_second(half, 2)
    for half in range(2):
        for side in SIDES:
            rows = sum_rows(sum_block(half, 0, 2), part_start(half, side), PART)
            send(slot("G1", half, side), part.at[rows, :], second1.at[half, which(side)], g_device(half, side))

    def mine(n, carried):
        weight_part(wrap(y + pick(n, ahead)) * 2 + core)
        return carried

    lax.fori_loop(0, RING, mine, 0)
    for n in range(RING):
        chunk = wrap(y + ahead[n]) * 2 + core
        arrived(slot("pair", n), pair1.at[n])
        wg[chunk] = (wg[chunk].astype(F32) + pair1[n].astype(F32)).astype(BF16)
        if n == 0:
            for side in SIDES:
                rows = pl.ds(0 if side == 1 else BLOCK, BLOCK)
                send(slot("Y1", side), wg.at[chunk, rows, :], ring1.at[which(side)], along_y(side))

    for j in (1, 3):
        for half in range(2):
            take_second(half, j)

    for side in SIDES:
        chunk = wrap(y + side) * 2 + core
        rows = pl.ds(0 if side == 1 else BLOCK, BLOCK)
        arrived(slot("Y1", side), ring1.at[which(side)])
        wg[chunk, rows, :] = (wg[chunk, rows, :].astype(F32) + ring1[which(side)].astype(F32)).astype(BF16)
        send(slot("Y2", side), wg.at[chunk], ring2.at[which(side)], along_y(side))

    for half in range(2):
        for side in SIDES:
            block = sum_block(half, 0, side)
            arrived(slot("G1", half, side), second1.at[half, which(side)])
            add_into(part, sum_rows(block, part_start(half, side), PART), [second1[half, which(side)]])
            rows = sum_rows(block, half * HALF, HALF)
            send(slot("G2", half, side), part.at[rows, :], second2.at[half, which(side)], g_device(half, side))

    for half in range(2):
        take_second(half, 0)

    for side in SIDES:
        arrived(slot("Y2", side), ring2.at[which(side)])
    total = (wg[y * 2 + core].astype(F32) + ring2[0].astype(F32) + ring2[1].astype(F32)) * (1.0 / (2 * RING))
    out_q[...] = total[:, 0:head]
    out_k[...] = total[:, head : 2 * head]
    out_v[...] = total[:, 2 * head : 3 * head]

    for half in range(2):
        for side in SIDES:
            arrived(slot("G2", half, side), second2.at[half, which(side)])
        rows = sum_rows(sp, half * HALF, HALF)
        total = part[rows, :].astype(F32) + second2[half, 0].astype(F32) + second2[half, 1].astype(F32)
        out_x[0, half * HALF : (half + 1) * HALF, :] = total.astype(BF16)

    for index, source in sent:
        copy(index, source, source, partner).wait_send()


A2A_ORDER = (1, 15, 4, 12, 3, 5, 11, 13, 2, 14, 8, 6, 7, 9, 10)
COPIES = 160


def body(hidden_in, mix_cotangent, query_weight, key_weight, value_weight, decay_log):
    depth = hidden_in.shape[2]
    head = query_weight.shape[1]
    blocks = RING * RING
    length = blocks * BLOCK
    wide = 3 * head
    vmem = pl.BlockSpec(memory_space=pltpu.VMEM)
    anywhere = pl.BlockSpec(memory_space=pl.ANY)
    return pl.pallas_call(
        all_kernel,
        out_shape=(
            jax.ShapeDtypeStruct(hidden_in.shape, BF16),
            jax.ShapeDtypeStruct((head, head), F32),
            jax.ShapeDtypeStruct((head, head), F32),
            jax.ShapeDtypeStruct((head, head), F32),
        ),
        in_specs=[pl.BlockSpec(memory_space=pltpu.SMEM)] + [anywhere] * 5,
        out_specs=(vmem,) * 4,
        scratch_shapes=[
            pltpu.VMEM((length, depth), BF16),
            pltpu.VMEM((depth, wide), BF16),
            pltpu.VMEM((length, wide), BF16),
            pltpu.VMEM((length, head), BF16),
            pltpu.VMEM((length, wide), F32),
            pltpu.VMEM((BLOCK, BLOCK), F32),
            pltpu.VMEM((BLOCK, BLOCK), F32),
            pltpu.VMEM((BLOCK, head), F32),
            pltpu.VMEM((BLOCK, head), F32),
            pltpu.VMEM((blocks, head, head), F32),
            pltpu.VMEM((blocks, head, head), F32),
            pltpu.VMEM((blocks, head, head), BF16),
            pltpu.VMEM((blocks, head, head), BF16),
            pltpu.VMEM((length, wide), BF16),
            pltpu.VMEM((length, depth), BF16),
            pltpu.VMEM((2, 2, RING, PART, depth), BF16),
            pltpu.VMEM((2, 2, RING, HALF, depth), BF16),
            pltpu.VMEM((2, 2, PART, depth), BF16),
            pltpu.VMEM((2, 2, HALF, depth), BF16),
            pltpu.VMEM((2 * RING, depth // (2 * RING), wide), BF16),
            pltpu.VMEM((RING, depth // (2 * RING), wide), BF16),
            pltpu.VMEM((2, depth // (4 * RING), wide), BF16),
            pltpu.VMEM((2, depth // (2 * RING), wide), BF16),
            pltpu.SemaphoreType.DMA((5,)),
            pltpu.SemaphoreType.DMA((COPIES,)),
            pltpu.SemaphoreType.DMA((COPIES,)),
        ],
        compiler_params=pltpu.CompilerParams(
            vmem_limit_bytes=67043328, collective_id=0, has_side_effects=True
        ),
        cost_estimate=pl.CostEstimate(flops=21 * 10**9, bytes_accessed=4 * 10**6, transcendentals=0),
    )(decay_log, hidden_in, mix_cotangent, query_weight, key_weight, value_weight)


def solution(mesh):
    placed = (P("dp", "sp", None), P("dp", "sp", None), P("dp", "sp"), P("dp", "sp"), P("dp", "sp"), P("sp"))
    return jax.shard_map(
        body,
        mesh=mesh,
        in_specs=placed,
        out_specs=(P("dp", "sp", None), P("dp", "sp"), P("dp", "sp"), P("dp", "sp")),
        check_vma=False,
    )
```

```python
import jax
import jax.numpy as jnp
from jax import lax
from jax.experimental import pallas as pl
from jax.experimental.pallas import tpu as pltpu
from jax.sharding import PartitionSpec as P

BLOCK = 128
HALF = 64
PART = 32
RING = 4
F32 = jnp.float32
BF16 = jnp.bfloat16
MESH = pl.DeviceIdType.MESH
SIDES = (1, -1)


def dot(a, b):
    return lax.dot_general(a, b, (((1,), (0,)), ((), ())), preferred_element_type=F32)


def dot_t(a, b):
    return lax.dot_general(a, b, (((1,), (1,)), ((), ())), preferred_element_type=F32)


def t_dot(a, b):
    return lax.dot_general(a, b, (((0,), (0,)), ((), ())), preferred_element_type=F32)


def rows_of(block):
    return pl.ds(pl.multiple_of(block * BLOCK, BLOCK), BLOCK)


def pick(index, values):
    got = jnp.int32(values[-1])
    for place, value in enumerate(values[:-1]):
        got = jnp.where(index == place, jnp.int32(value), got)
    return got


def add_into(target, rows, others):
    total = target[rows, :].astype(F32)
    for other in others:
        total = total + other.astype(F32)
    target[rows, :] = total.astype(BF16)


def make_decays(rate, inner_ref, inner_t_ref, query_ref, key_ref):
    row = lax.broadcasted_iota(jnp.int32, (BLOCK, BLOCK), 0)
    col = lax.broadcasted_iota(jnp.int32, (BLOCK, BLOCK), 1)
    spread = (row - col).astype(F32)
    inner_ref[...] = jnp.where(spread >= 0, jnp.exp(rate * jnp.maximum(spread, 0.0)), 0.0)
    inner_t_ref[...] = jnp.where(spread <= 0, jnp.exp(rate * jnp.maximum(-spread, 0.0)), 0.0)
    offset = lax.broadcasted_iota(jnp.int32, query_ref.shape, 0).astype(F32)
    query_ref[...] = jnp.exp(rate * (offset + 1.0))
    key_ref[...] = jnp.exp(rate * (BLOCK - 1.0 - offset))


def in_block(block, head, scale, qkv, cot, decays, grads, fwd_states, bwd_states):
    inner_ref, inner_t_ref, query_ref, key_ref = decays
    rows = rows_of(block)
    queries = qkv[rows, 0:head]
    keys = qkv[rows, head : 2 * head]
    values = qkv[rows, 2 * head : 3 * head]
    given = cot[rows, :]
    mixed = (dot_t(given, values) * inner_ref[...]).astype(BF16)
    grads[rows, 0:head] = dot(mixed, keys)
    mixed_t = (dot_t(values, given) * inner_t_ref[...]).astype(BF16)
    grads[rows, head : 2 * head] = dot(mixed_t, queries) * scale
    scores_t = (dot_t(keys, queries) * inner_t_ref[...]).astype(BF16)
    grads[rows, 2 * head : 3 * head] = dot(scores_t, given)
    keys_w = (keys.astype(F32) * key_ref[...]).astype(BF16)
    fwd_states[block] = t_dot(keys_w, values)
    queries_w = (queries.astype(F32) * query_ref[...]).astype(BF16)
    bwd_states[block] = t_dot(queries_w, given)


def run_states(rate, blocks, fwd_states, bwd_states, fwd_bf, bwd_bf):
    size = 32
    wide = fwd_states.shape[2]
    step = jnp.exp(jnp.full((size, wide), BLOCK, F32) * rate)

    def chunk(n, carried):
        rows = pl.ds(pl.multiple_of(n * size, size), size)
        ahead = jnp.zeros((size, wide), F32)
        back = jnp.zeros((size, wide), F32)
        for i in range(blocks):
            fwd_bf[i, rows, :] = ahead.astype(BF16)
            ahead = ahead * step + fwd_states[i, rows, :]
            last = blocks - 1 - i
            bwd_bf[last, rows, :] = back.astype(BF16)
            back = back * step + bwd_states[last, rows, :]
        return carried

    lax.fori_loop(0, fwd_states.shape[1] // size, chunk, 0)


def cross_block(block, head, scale, qkv, cot, decays, grads, fwd_bf, bwd_bf, out):
    _, _, query_ref, key_ref = decays
    rows = rows_of(block)
    keys = qkv[rows, head : 2 * head]
    values = qkv[rows, 2 * head : 3 * head]
    state = fwd_bf[block]
    back = bwd_bf[block]
    grad_q = grads[rows, 0:head] + dot_t(cot[rows, :], state) * query_ref[...]
    grad_k = grads[rows, head : 2 * head] + dot_t(values, back) * (key_ref[...] * scale)
    grad_v = grads[rows, 2 * head : 3 * head] + dot(keys, back) * key_ref[...]
    out[rows, 0:head] = grad_q.astype(BF16)
    out[rows, head : 2 * head] = grad_k.astype(BF16)
    out[rows, 2 * head : 3 * head] = grad_v.astype(BF16)


def all_kernel(
    rate_ref,
    own_x,
    own_cot,
    wq_ref,
    wk_ref,
    wv_ref,
    out_x,
    out_w,
    xall,
    w,
    qkv,
    cot,
    grads,
    inner,
    inner_t,
    query_d,
    key_d,
    fwd,
    bwd,
    fwd_bf,
    bwd_bf,
    g,
    part,
    first1,
    first2,
    second1,
    second2,
    wg,
    pair1,
    ring1,
    ring2,
    local_sem,
    send_sem,
    recv_sem,
):
    depth = xall.shape[1]
    head = cot.shape[1]
    blocks = RING * RING
    scale = head ** (-0.5)
    sp = lax.axis_index("sp")
    dp = lax.axis_index("dp")
    z, x = lax.div(sp, RING), lax.rem(sp, RING)
    y, core = lax.div(dp, 2), lax.rem(dp, 2)
    rate = rate_ref[0]
    decays = (inner, inner_t, query_d, key_d)
    names = {}
    sent = []

    def slot(*name):
        return names.setdefault(name, len(names))

    def slots(count, *name):
        first = slot(*name, 0)
        for place in range(1, count):
            assert slot(*name, place) == first + place
        return first

    def wrap(value):
        return lax.rem(value + RING, RING)

    def block_at(dz, dx):
        return wrap(z + dz) * RING + wrap(x + dx)

    def plane(dz, dx):
        return (block_at(dz, dx), dp)

    def along_y(dy):
        return (sp, wrap(y + dy) * 2 + core)

    partner = (sp, y * 2 + 1 - core)

    def along(half, first, second):
        return (second, first) if half == 0 else (first, second)

    def copy(index, source, target, device):
        return pltpu.make_async_remote_copy(
            src_ref=source,
            dst_ref=target,
            send_sem=send_sem.at[index],
            recv_sem=recv_sem.at[index],
            device_id=device,
            device_id_type=MESH,
        )

    def send(index, source, target, device):
        copy(index, source, target, device).start()
        sent.append((index, source))

    def send_in_loop(index, source, target, device):
        copy(index, source, target, device).start()

    def arrived(index, target):
        copy(index, target, target, partner).wait_recv()

    barrier = pltpu.get_barrier_semaphore()
    friends = [plane(dz, dx) for dz in range(RING) for dx in range(RING) if dz or dx]
    friends = friends + [along_y(1), along_y(-1), partner]
    for friend in friends:
        pl.semaphore_signal(barrier, inc=1, device_id=friend, device_id_type=MESH)

    own_rows = rows_of(sp)
    w_rows = pl.ds(pl.multiple_of(dp * head, head), head)
    loads = [
        pltpu.make_async_copy(own_x.at[0], xall.at[own_rows, :], local_sem.at[0]),
        pltpu.make_async_copy(wq_ref, w.at[w_rows, 0:head], local_sem.at[1]),
        pltpu.make_async_copy(wk_ref, w.at[w_rows, head : 2 * head], local_sem.at[2]),
        pltpu.make_async_copy(wv_ref, w.at[w_rows, 2 * head : 3 * head], local_sem.at[3]),
        pltpu.make_async_copy(
            own_cot.at[0, :, pl.ds(pl.multiple_of(sp * head, head), head)], cot.at[own_rows, :], local_sem.at[4]
        ),
    ]
    for load in loads:
        load.start()
    make_decays(rate, *decays)
    for load in loads:
        load.wait()
    pl.semaphore_wait(barrier, len(friends))

    def x_rows(block, start, count):
        return xall.at[pl.ds(pl.multiple_of(block * BLOCK + start, PART), count), :]

    def part_start(half, side):
        return half * HALF + (0 if side == 1 else PART)

    def gather_block(half, p, q):
        return block_at(*along(half, p, q))

    def gather_send(name, half, p, q, side, axis):
        block = gather_block(half, p, q)
        if name[0] in ("s1", "s2"):
            rows = x_rows(block, half * HALF, HALF)
        else:
            rows = x_rows(block, part_start(half, side), PART)
        device = plane(*along(half, side, 0)) if axis == 0 else plane(*along(half, 0, side))
        send(slot(*name), rows, rows, device)

    def gather_wait(name, half, p, q, side):
        block = gather_block(half, p, q)
        if name[0] in ("s1", "s2"):
            rows = x_rows(block, half * HALF, HALF)
        else:
            rows = x_rows(block, part_start(half, side), PART)
        arrived(slot(*name), rows)

    def w_part(dy, which, start, count):
        first = (wrap(y + dy) * 2 + which) * head
        return w.at[pl.ds(pl.multiple_of(first + start, BLOCK), count), :]

    for half in range(2):
        for side in SIDES:
            gather_send(("s1", half, side), half, 0, 0, side, 0)
    for side in SIDES:
        send(slot("w1", side), w_part(0, core, 0, head), w_part(0, core, 0, head), along_y(side))
    send(slot("wc", 0), w_part(0, core, 0, head), w_part(0, core, 0, head), partner)
    for half in range(2):
        for side in SIDES:
            gather_send(("s2", half, 0, side), half, 0, 0, side, 1)
    for offset in A2A_ORDER:
        target = lax.rem(sp + offset, blocks)
        send(
            slot("cot", offset),
            own_cot.at[0, :, pl.ds(pl.multiple_of(target * head, head), head)],
            cot.at[own_rows, :],
            (target, dp),
        )

    def project(block):
        rows = rows_of(block)
        got = dot(xall[rows, :], w[...])
        qkv[rows, 0:head] = got[:, 0:head].astype(BF16)
        qkv[rows, head : 2 * head] = (got[:, head : 2 * head].astype(BF16).astype(F32) * scale).astype(BF16)
        qkv[rows, 2 * head : 3 * head] = got[:, 2 * head : 3 * head].astype(BF16)

    def inside(block):
        in_block(block, head, scale, qkv, cot, decays, grads, fwd, bwd)

    def loop(places, *works):
        def step(n, carried):
            block = block_at(pick(n, [dz for dz, _ in places]), pick(n, [dx for _, dx in places]))
            for work in works:
                work(block)
            return carried

        lax.fori_loop(0, len(places), step, 0)

    near = [(0, 0), (0, 1), (0, 3), (1, 0), (3, 0)]
    corners = [(1, 1), (1, 3), (3, 1), (3, 3)]
    far = [(0, 2), (2, 0)]
    last = [(2, 2)]

    for half in range(2):
        for side in SIDES:
            gather_wait(("s1", half, side), half, -side, 0, side)
            gather_send(("f1", half, side), half, -side, 0, side, 0)
    for half in range(2):
        for near_p in SIDES:
            for side in SIDES:
                gather_send(("s2", half, near_p, side), half, near_p, 0, side, 1)

    for side in SIDES:
        arrived(slot("w1", side), w_part(-side, core, 0, head))
        rows = w_part(-side, core, 0 if side == 1 else BLOCK, BLOCK)
        send(slot("w2", side), rows, rows, along_y(side))
        rows = w_part(-side, core, 0, head)
        send(slot("wc", side), rows, rows, partner)

    for half in range(2):
        for side in SIDES:
            gather_wait(("s2", half, 0, side), half, 0, -side, side)
            gather_send(("f2", half, 0, side), half, 0, -side, side, 1)

    for side in SIDES:
        arrived(slot("w2", side), w_part(2, core, 0 if side == 1 else BLOCK, BLOCK))
    send(slot("wc", 2), w_part(2, core, 0, head), w_part(2, core, 0, head), partner)
    for dy in (0, 1, -1, 2):
        arrived(slot("wc", dy), w_part(-dy, 1 - core, 0, head))

    loop(near, project)

    for half in range(2):
        for side in SIDES:
            gather_wait(("f1", half, side), half, 2, 0, side)
    for half in range(2):
        for side in SIDES:
            gather_send(("s2", half, 2, side), half, 2, 0, side, 1)

    for offset in A2A_ORDER:
        arrived(slot("cot", offset), cot.at[rows_of(lax.rem(sp + blocks - offset, blocks)), :])
    loop(near, inside)

    for near_p in SIDES:
        for half in range(2):
            for side in SIDES:
                gather_wait(("s2", half, near_p, side), half, near_p, -side, side)
                gather_send(("f2", half, near_p, side), half, near_p, -side, side, 1)
    loop(corners, project, inside)

    for half in range(2):
        for side in SIDES:
            gather_wait(("f2", half, 0, side), half, 0, 2, side)
    loop(far, project, inside)

    for half in range(2):
        for side in SIDES:
            gather_wait(("s2", half, 2, side), half, 2, -side, side)
            gather_send(("f2", half, 2, side), half, 2, -side, side, 1)

    for near_p in SIDES:
        for half in range(2):
            for side in SIDES:
                gather_wait(("f2", half, near_p, side), half, near_p, 2, side)
        loop([(2, near_p), (near_p, 2)], project, inside)

    for half in range(2):
        for side in SIDES:
            gather_wait(("f2", half, 2, side), half, 2, 2, side)
    loop(last, project, inside)

    run_states(rate, blocks, fwd, bwd, fwd_bf, bwd_bf)

    def finish(block):
        cross_block(block, head, scale, qkv, cot, decays, grads, fwd_bf, bwd_bf, g)
        rows = rows_of(block)
        part[rows, :] = dot_t(g[rows, :], w[...]).astype(BF16)

    def sum_block(half, f, q):
        return block_at(*((f, q) if half == 0 else (q, f)))

    def sum_rows(block, start, count):
        return pl.ds(pl.multiple_of(block * BLOCK + start, PART), count)

    def f_device(half, side):
        return plane(side, 0) if half == 0 else plane(0, side)

    def g_device(half, side):
        return plane(0, side) if half == 0 else plane(side, 0)

    def which(side):
        return 0 if side == 1 else 1

    firsts = {(half, side): slots(RING, "F1", half, side) for half in range(2) for side in SIDES}

    def send_first(half, j):
        for side in SIDES:
            rows = sum_rows(sum_block(half, 2, j), part_start(half, side), PART)
            send_in_loop(
                firsts[half, side] + j, part.at[rows, :], first1.at[half, which(side), j], f_device(half, side)
            )

    def send_second(half, j):
        for side in SIDES:
            block = sum_block(half, side, j)
            rows = sum_rows(block, part_start(half, side), PART)
            arrived(firsts[half, side] + j, first1.at[half, which(side), j])
            add_into(part, rows, [first1[half, which(side), j]])
        for side in SIDES:
            block = sum_block(half, side, j)
            rows = sum_rows(block, half * HALF, HALF)
            send(slot("F2", half, j, side), part.at[rows, :], first2.at[half, which(side), j], f_device(half, side))

    def take_second(half, j):
        for side in SIDES:
            arrived(slot("F2", half, j, side), first2.at[half, which(side), j])
        rows = sum_rows(sum_block(half, 0, j), half * HALF, HALF)
        add_into(part, rows, [first2[half, 0, j], first2[half, 1, j]])

    finish(block_at(2, 2))
    for half in range(2):
        send_first(half, 2)

    def outer(n, carried):
        place = pick(n, (1, 3, 0))
        finish(block_at(2, place))
        finish(block_at(place, 2))
        for half in range(2):
            send_first(half, place)
        return carried

    lax.fori_loop(0, 3, outer, 0)
    for half in range(2):
        send_second(half, 2)
    loop(corners, finish)
    for j in (1, 3):
        for half in range(2):
            send_second(half, j)
    loop([(1, 0), (3, 0), (0, 1), (0, 3), (0, 0)], finish)

    ahead = (2, 1, 3, 0)

    def weight_parts(n):
        first = wrap(y + ahead[n]) * 2

        def step(i, carried):
            chunk = first + jnp.where(i == 0, 1 - core, core)
            columns = pl.ds(pl.multiple_of(chunk * head, head), head)
            wg[chunk] = t_dot(xall[:, columns], g[...]).astype(BF16)
            return carried

        lax.fori_loop(0, 2, step, 0)
        send(slot("pair", n), wg.at[first + 1 - core], pair1.at[n], partner)

    def add_pair(n):
        chunk = wrap(y + ahead[n]) * 2 + core
        arrived(slot("pair", n), pair1.at[n])
        wg[chunk] = (wg[chunk].astype(F32) + pair1[n].astype(F32)).astype(BF16)

    weight_parts(0)
    for half in range(2):
        take_second(half, 2)
    for half in range(2):
        for side in SIDES:
            rows = sum_rows(sum_block(half, 0, 2), part_start(half, side), PART)
            send(slot("G1", half, side), part.at[rows, :], second1.at[half, which(side)], g_device(half, side))
    for half in range(2):
        send_second(half, 0)

    weight_parts(1)
    add_pair(0)
    for side in SIDES:
        chunk = wrap(y + 2) * 2 + core
        rows = pl.ds(0 if side == 1 else BLOCK, BLOCK)
        send(slot("Y1", side), wg.at[chunk, rows, :], ring1.at[which(side)], along_y(side))
    weight_parts(2)
    add_pair(1)
    weight_parts(3)
    add_pair(2)
    for side in SIDES:
        chunk = wrap(y + side) * 2 + core
        rows = pl.ds(0 if side == 1 else BLOCK, BLOCK)
        arrived(slot("Y1", side), ring1.at[which(side)])
        wg[chunk, rows, :] = (wg[chunk, rows, :].astype(F32) + ring1[which(side)].astype(F32)).astype(BF16)
        send(slot("Y2", side), wg.at[chunk], ring2.at[which(side)], along_y(side))
    add_pair(3)

    for j in (1, 3):
        for half in range(2):
            take_second(half, j)
    for half in range(2):
        for side in SIDES:
            block = sum_block(half, 0, side)
            arrived(slot("G1", half, side), second1.at[half, which(side)])
            add_into(part, sum_rows(block, part_start(half, side), PART), [second1[half, which(side)]])
            rows = sum_rows(block, half * HALF, HALF)
            send(slot("G2", half, side), part.at[rows, :], second2.at[half, which(side)], g_device(half, side))

    for half in range(2):
        take_second(half, 0)

    for side in SIDES:
        arrived(slot("Y2", side), ring2.at[which(side)])
    out_w[...] = wg[y * 2 + core].astype(F32) + ring2[0].astype(F32) + ring2[1].astype(F32)

    for half in range(2):
        for side in SIDES:
            arrived(slot("G2", half, side), second2.at[half, which(side)])
        rows = sum_rows(sp, half * HALF, HALF)
        total = part[rows, :].astype(F32) + second2[half, 0].astype(F32) + second2[half, 1].astype(F32)
        out_x[0, half * HALF : (half + 1) * HALF, :] = total.astype(BF16)

    for half in range(2):
        for side in SIDES:
            for j in range(RING):
                source = first1.at[half, which(side), j]
                copy(firsts[half, side] + j, source, source, partner).wait_send()
    for index, source in sent:
        copy(index, source, source, partner).wait_send()


A2A_ORDER = (1, 15, 4, 12, 3, 5, 11, 13, 2, 14, 8, 6, 7, 9, 10)
COPIES = 160
VMEM_LIMIT = 67043328


def split_kernel(sum_x, sum_w, out_x, out_q, out_k, out_v):
    head = out_q.shape[1]
    out_x[...] = sum_x[...]
    for place, out in enumerate((out_q, out_k, out_v)):
        out[...] = sum_w[:, place * head : (place + 1) * head] * (1.0 / (2 * RING))


def body(hidden_in, mix_cotangent, query_weight, key_weight, value_weight, decay_log):
    depth = hidden_in.shape[2]
    head = query_weight.shape[1]
    blocks = RING * RING
    length = blocks * BLOCK
    wide = 3 * head
    vmem = pl.BlockSpec(memory_space=pltpu.VMEM)
    anywhere = pl.BlockSpec(memory_space=pl.ANY)
    sum_x, sum_w = pl.pallas_call(
        all_kernel,
        out_shape=(
            jax.ShapeDtypeStruct(hidden_in.shape, BF16),
            jax.ShapeDtypeStruct((head, wide), F32),
        ),
        in_specs=[pl.BlockSpec(memory_space=pltpu.SMEM)] + [anywhere] * 5,
        out_specs=(vmem,) * 2,
        scratch_shapes=[
            pltpu.VMEM((length, depth), BF16),
            pltpu.VMEM((depth, wide), BF16),
            pltpu.VMEM((length, wide), BF16),
            pltpu.VMEM((length, head), BF16),
            pltpu.VMEM((length, wide), F32),
            pltpu.VMEM((BLOCK, BLOCK), F32),
            pltpu.VMEM((BLOCK, BLOCK), F32),
            pltpu.VMEM((BLOCK, head), F32),
            pltpu.VMEM((BLOCK, head), F32),
            pltpu.VMEM((blocks, head, head), F32),
            pltpu.VMEM((blocks, head, head), F32),
            pltpu.VMEM((blocks, head, head), BF16),
            pltpu.VMEM((blocks, head, head), BF16),
            pltpu.VMEM((length, wide), BF16),
            pltpu.VMEM((length, depth), BF16),
            pltpu.VMEM((2, 2, RING, PART, depth), BF16),
            pltpu.VMEM((2, 2, RING, HALF, depth), BF16),
            pltpu.VMEM((2, 2, PART, depth), BF16),
            pltpu.VMEM((2, 2, HALF, depth), BF16),
            pltpu.VMEM((2 * RING, depth // (2 * RING), wide), BF16),
            pltpu.VMEM((RING, depth // (2 * RING), wide), BF16),
            pltpu.VMEM((2, depth // (4 * RING), wide), BF16),
            pltpu.VMEM((2, depth // (2 * RING), wide), BF16),
            pltpu.SemaphoreType.DMA((5,)),
            pltpu.SemaphoreType.DMA((COPIES,)),
            pltpu.SemaphoreType.DMA((COPIES,)),
        ],
        compiler_params=pltpu.CompilerParams(
            vmem_limit_bytes=VMEM_LIMIT, collective_id=0, has_side_effects=True
        ),
        cost_estimate=pl.CostEstimate(flops=21 * 10**9, bytes_accessed=4 * 10**6, transcendentals=0),
    )(decay_log, hidden_in, mix_cotangent, query_weight, key_weight, value_weight)
    return pl.pallas_call(
        split_kernel,
        out_shape=(
            jax.ShapeDtypeStruct(hidden_in.shape, BF16),
            jax.ShapeDtypeStruct((head, head), F32),
            jax.ShapeDtypeStruct((head, head), F32),
            jax.ShapeDtypeStruct((head, head), F32),
        ),
        in_specs=[vmem] * 2,
        out_specs=(vmem,) * 4,
    )(sum_x, sum_w)


def solution(mesh):
    placed = (P("dp", "sp", None), P("dp", "sp", None), P("dp", "sp"), P("dp", "sp"), P("dp", "sp"), P("sp"))
    return jax.shard_map(
        body,
        mesh=mesh,
        in_specs=placed,
        out_specs=(P("dp", "sp", None), P("dp", "sp"), P("dp", "sp"), P("dp", "sp")),
        check_vma=False,
    )
```

```python
import jax
import jax.numpy as jnp
from jax import lax
from jax.experimental import pallas as pl
from jax.experimental.pallas import tpu as pltpu
from jax.sharding import PartitionSpec as P

BLOCK = 128
HALF = 64
PART = 32
RING = 4
F32 = jnp.float32
BF16 = jnp.bfloat16
MESH = pl.DeviceIdType.MESH
SIDES = (1, -1)


def dot(a, b):
    return lax.dot_general(a, b, (((1,), (0,)), ((), ())), preferred_element_type=F32)


def dot_t(a, b):
    return lax.dot_general(a, b, (((1,), (1,)), ((), ())), preferred_element_type=F32)


def t_dot(a, b):
    return lax.dot_general(a, b, (((0,), (0,)), ((), ())), preferred_element_type=F32)


def rows_of(block):
    return pl.ds(pl.multiple_of(block * BLOCK, BLOCK), BLOCK)


def pick(index, values):
    got = jnp.int32(values[-1])
    for place, value in enumerate(values[:-1]):
        got = jnp.where(index == place, jnp.int32(value), got)
    return got


def add_into(target, rows, others):
    total = target[rows, :].astype(F32)
    for other in others:
        total = total + other.astype(F32)
    target[rows, :] = total.astype(BF16)


def make_decays(rate, inner_ref, inner_t_ref, query_ref, key_ref):
    row = lax.broadcasted_iota(jnp.int32, (BLOCK, BLOCK), 0)
    col = lax.broadcasted_iota(jnp.int32, (BLOCK, BLOCK), 1)
    spread = (row - col).astype(F32)
    inner_ref[...] = jnp.where(spread >= 0, jnp.exp(rate * jnp.maximum(spread, 0.0)), 0.0)
    inner_t_ref[...] = jnp.where(spread <= 0, jnp.exp(rate * jnp.maximum(-spread, 0.0)), 0.0)
    offset = lax.broadcasted_iota(jnp.int32, query_ref.shape, 0).astype(F32)
    query_ref[...] = jnp.exp(rate * (offset + 1.0))
    key_ref[...] = jnp.exp(rate * (BLOCK - 1.0 - offset))


def in_block(block, head, scale, qkv, cot, decays, grads, fwd_states, bwd_states):
    inner_ref, inner_t_ref, query_ref, key_ref = decays
    rows = rows_of(block)
    queries = qkv[rows, 0:head]
    keys = qkv[rows, head : 2 * head]
    values = qkv[rows, 2 * head : 3 * head]
    given = cot[rows, :]
    mixed = (dot_t(given, values) * inner_ref[...]).astype(BF16)
    grads[rows, 0:head] = dot(mixed, keys)
    mixed_t = (dot_t(values, given) * inner_t_ref[...]).astype(BF16)
    grads[rows, head : 2 * head] = dot(mixed_t, queries) * scale
    scores_t = (dot_t(keys, queries) * inner_t_ref[...]).astype(BF16)
    grads[rows, 2 * head : 3 * head] = dot(scores_t, given)
    keys_w = (keys.astype(F32) * key_ref[...]).astype(BF16)
    fwd_states[block] = t_dot(keys_w, values)
    queries_w = (queries.astype(F32) * query_ref[...]).astype(BF16)
    bwd_states[block] = t_dot(queries_w, given)


def run_states(rate, blocks, fwd_states, bwd_states, fwd_bf, bwd_bf):
    size = 32
    wide = fwd_states.shape[2]
    step = jnp.exp(jnp.full((size, wide), BLOCK, F32) * rate)

    def chunk(n, carried):
        rows = pl.ds(pl.multiple_of(n * size, size), size)
        ahead = jnp.zeros((size, wide), F32)
        back = jnp.zeros((size, wide), F32)
        for i in range(blocks):
            fwd_bf[i, rows, :] = ahead.astype(BF16)
            ahead = ahead * step + fwd_states[i, rows, :]
            last = blocks - 1 - i
            bwd_bf[last, rows, :] = back.astype(BF16)
            back = back * step + bwd_states[last, rows, :]
        return carried

    lax.fori_loop(0, fwd_states.shape[1] // size, chunk, 0)


def cross_block(block, head, scale, qkv, cot, decays, grads, fwd_bf, bwd_bf, out):
    _, _, query_ref, key_ref = decays
    rows = rows_of(block)
    keys = qkv[rows, head : 2 * head]
    values = qkv[rows, 2 * head : 3 * head]
    state = fwd_bf[block]
    back = bwd_bf[block]
    grad_q = grads[rows, 0:head] + dot_t(cot[rows, :], state) * query_ref[...]
    grad_k = grads[rows, head : 2 * head] + dot_t(values, back) * (key_ref[...] * scale)
    grad_v = grads[rows, 2 * head : 3 * head] + dot(keys, back) * key_ref[...]
    out[rows, 0:head] = grad_q.astype(BF16)
    out[rows, head : 2 * head] = grad_k.astype(BF16)
    out[rows, 2 * head : 3 * head] = grad_v.astype(BF16)


def all_kernel(
    rate_ref,
    own_x,
    own_cot,
    wq_ref,
    wk_ref,
    wv_ref,
    out_x,
    out_w,
    xall,
    w,
    qkv,
    cot,
    grads,
    inner,
    inner_t,
    query_d,
    key_d,
    fwd,
    bwd,
    fwd_bf,
    bwd_bf,
    g,
    part,
    first1,
    first2,
    second1,
    second2,
    wg,
    pair1,
    ring1,
    ring2,
    local_sem,
    send_sem,
    recv_sem,
    ready_sem,
    rate_smem,
    done_x,
    done_w,
):
    depth = xall.shape[1]
    head = cot.shape[1]
    blocks = RING * RING
    scale = head ** (-0.5)
    sp = lax.axis_index("sp")
    dp = lax.axis_index("dp")
    z, x = lax.div(sp, RING), lax.rem(sp, RING)
    y, core = lax.div(dp, 2), lax.rem(dp, 2)
    decays = (inner, inner_t, query_d, key_d)
    names = {}
    sent = []

    def slot(*name):
        return names.setdefault(name, len(names))

    def slots(count, *name):
        first = slot(*name, 0)
        for place in range(1, count):
            assert slot(*name, place) == first + place
        return first

    def wrap(value):
        return lax.rem(value + RING, RING)

    def block_at(dz, dx):
        return wrap(z + dz) * RING + wrap(x + dx)

    def plane(dz, dx):
        return (block_at(dz, dx), dp)

    def along_y(dy):
        return (sp, wrap(y + dy) * 2 + core)

    partner = (sp, y * 2 + 1 - core)

    def along(half, first, second):
        return (second, first) if half == 0 else (first, second)

    def copy(index, source, target, device):
        return pltpu.make_async_remote_copy(
            src_ref=source,
            dst_ref=target,
            send_sem=send_sem.at[index],
            recv_sem=recv_sem.at[index],
            device_id=device,
            device_id_type=MESH,
        )

    def send(index, source, target, device):
        copy(index, source, target, device).start()
        sent.append((index, source))

    def send_in_loop(index, source, target, device):
        copy(index, source, target, device).start()

    def arrived(index, target):
        copy(index, target, target, partner).wait_recv()

    barrier = pltpu.get_barrier_semaphore()
    beside = [plane(0, 1), plane(0, -1), plane(1, 0), plane(-1, 0)]
    friends = beside + [along_y(1), along_y(-1), partner]
    for friend in friends:
        pl.semaphore_signal(barrier, inc=1, device_id=friend, device_id_type=MESH)

    own_rows = rows_of(sp)
    w_rows = pl.ds(pl.multiple_of(dp * head, head), head)
    loads = [
        pltpu.make_async_copy(own_x.at[0], xall.at[own_rows, :], local_sem.at[0]),
        pltpu.make_async_copy(wq_ref, w.at[w_rows, 0:head], local_sem.at[1]),
        pltpu.make_async_copy(wk_ref, w.at[w_rows, head : 2 * head], local_sem.at[2]),
        pltpu.make_async_copy(wv_ref, w.at[w_rows, 2 * head : 3 * head], local_sem.at[3]),
        pltpu.make_async_copy(
            own_cot.at[0, :, pl.ds(pl.multiple_of(sp * head, head), head)], cot.at[own_rows, :], local_sem.at[4]
        ),
    ]
    loads.append(pltpu.make_async_copy(rate_ref, rate_smem, local_sem.at[5]))
    for load in loads:
        load.start()
    for load in loads:
        load.wait()
    rate = rate_smem[0]
    pl.semaphore_wait(barrier, len(friends))

    def x_rows(block, start, count):
        return xall.at[pl.ds(pl.multiple_of(block * BLOCK + start, PART), count), :]

    def part_start(half, side):
        return half * HALF + (0 if side == 1 else PART)

    def gather_block(half, p, q):
        return block_at(*along(half, p, q))

    def gather_send(name, half, p, q, side, axis):
        block = gather_block(half, p, q)
        if name[0] in ("s1", "s2"):
            rows = x_rows(block, half * HALF, HALF)
        else:
            rows = x_rows(block, part_start(half, side), PART)
        device = plane(*along(half, side, 0)) if axis == 0 else plane(*along(half, 0, side))
        send(slot(*name), rows, rows, device)

    def gather_wait(name, half, p, q, side):
        block = gather_block(half, p, q)
        if name[0] in ("s1", "s2"):
            rows = x_rows(block, half * HALF, HALF)
        else:
            rows = x_rows(block, part_start(half, side), PART)
        arrived(slot(*name), rows)

    def w_part(dy, which, start, count):
        first = (wrap(y + dy) * 2 + which) * head
        return w.at[pl.ds(pl.multiple_of(first + start, BLOCK), count), :]

    for side in SIDES:
        send(slot("w1", side), w_part(0, core, 0, head), w_part(0, core, 0, head), along_y(side))
    send(slot("wc", 0), w_part(0, core, 0, head), w_part(0, core, 0, head), partner)

    @pl.when(core == LATER)
    def _():
        pl.semaphore_wait(ready_sem.at[3], 1)

    for half in range(2):
        for side in SIDES:
            gather_send(("s1", half, side), half, 0, 0, side, 0)
    for half in range(2):
        for side in SIDES:
            gather_send(("s2", half, 0, side), half, 0, 0, side, 1)
    for turn in range(3):
        for friend in beside:
            pl.semaphore_signal(ready_sem.at[turn], inc=1, device_id=friend, device_id_type=MESH)
        pl.semaphore_wait(ready_sem.at[turn], len(beside))
    for offset in A2A_ORDER:
        target = lax.rem(sp + offset, blocks)
        send(
            slot("cot", offset),
            own_cot.at[0, :, pl.ds(pl.multiple_of(target * head, head), head)],
            cot.at[own_rows, :],
            (target, dp),
        )

    make_decays(rate, *decays)

    def project(block):
        rows = rows_of(block)
        got = dot(xall[rows, :], w[...])
        qkv[rows, 0:head] = got[:, 0:head].astype(BF16)
        qkv[rows, head : 2 * head] = (got[:, head : 2 * head].astype(BF16).astype(F32) * scale).astype(BF16)
        qkv[rows, 2 * head : 3 * head] = got[:, 2 * head : 3 * head].astype(BF16)

    def inside(block):
        in_block(block, head, scale, qkv, cot, decays, grads, fwd, bwd)

    def loop(places, *works):
        several = 2 if len(places) % 2 == 0 else 1

        def step(n, carried):
            group = []
            for m in range(several):
                at = n * several + m
                group.append(block_at(pick(at, [dz for dz, _ in places]), pick(at, [dx for _, dx in places])))
            for work in works:
                for block in group:
                    work(block)
            return carried

        lax.fori_loop(0, len(places) // several, step, 0)

    near = [(0, 0), (0, 1), (0, 3), (1, 0), (3, 0)]
    corners = [(1, 1), (1, 3), (3, 1), (3, 3)]
    far = [(0, 2), (2, 0)]
    last = [(2, 2)]

    for half in range(2):
        for side in SIDES:
            gather_wait(("s1", half, side), half, -side, 0, side)
            gather_send(("f1", half, side), half, -side, 0, side, 0)
    for half in range(2):
        for near_p in SIDES:
            for side in SIDES:
                gather_send(("s2", half, near_p, side), half, near_p, 0, side, 1)

    for side in SIDES:
        arrived(slot("w1", side), w_part(-side, core, 0, head))
        rows = w_part(-side, core, 0 if side == 1 else BLOCK, BLOCK)
        send(slot("w2", side), rows, rows, along_y(side))
        rows = w_part(-side, core, 0, head)
        send(slot("wc", side), rows, rows, partner)

    @pl.when(core != LATER)
    def _():
        pl.semaphore_signal(ready_sem.at[3], inc=1, device_id=partner, device_id_type=MESH)

    for half in range(2):
        for side in SIDES:
            gather_wait(("s2", half, 0, side), half, 0, -side, side)
            gather_send(("f2", half, 0, side), half, 0, -side, side, 1)

    for side in SIDES:
        arrived(slot("w2", side), w_part(2, core, 0 if side == 1 else BLOCK, BLOCK))
    send(slot("wc", 2), w_part(2, core, 0, head), w_part(2, core, 0, head), partner)
    for dy in (0, 1, -1, 2):
        arrived(slot("wc", dy), w_part(-dy, 1 - core, 0, head))

    loop(near, project)

    for half in range(2):
        for side in SIDES:
            gather_wait(("f1", half, side), half, 2, 0, side)
    for half in range(2):
        for side in SIDES:
            gather_send(("s2", half, 2, side), half, 2, 0, side, 1)

    for offset in A2A_ORDER:
        arrived(slot("cot", offset), cot.at[rows_of(lax.rem(sp + blocks - offset, blocks)), :])
    loop(near, inside)

    for near_p in SIDES:
        for half in range(2):
            for side in SIDES:
                gather_wait(("s2", half, near_p, side), half, near_p, -side, side)
                gather_send(("f2", half, near_p, side), half, near_p, -side, side, 1)
    loop(corners, project, inside)

    for half in range(2):
        for side in SIDES:
            gather_wait(("f2", half, 0, side), half, 0, 2, side)
    loop(far, project, inside)

    for half in range(2):
        for side in SIDES:
            gather_wait(("s2", half, 2, side), half, 2, -side, side)
            gather_send(("f2", half, 2, side), half, 2, -side, side, 1)

    for near_p in SIDES:
        for half in range(2):
            for side in SIDES:
                gather_wait(("f2", half, near_p, side), half, near_p, 2, side)
        loop([(2, near_p), (near_p, 2)], project, inside)

    for half in range(2):
        for side in SIDES:
            gather_wait(("f2", half, 2, side), half, 2, 2, side)
    loop(last, project, inside)

    run_states(rate, blocks, fwd, bwd, fwd_bf, bwd_bf)

    def finish(block):
        cross_block(block, head, scale, qkv, cot, decays, grads, fwd_bf, bwd_bf, g)
        rows = rows_of(block)
        part[rows, :] = dot_t(g[rows, :], w[...]).astype(BF16)

    def sum_block(half, f, q):
        return block_at(*((f, q) if half == 0 else (q, f)))

    def sum_rows(block, start, count):
        return pl.ds(pl.multiple_of(block * BLOCK + start, PART), count)

    def f_device(half, side):
        return plane(side, 0) if half == 0 else plane(0, side)

    def g_device(half, side):
        return plane(0, side) if half == 0 else plane(side, 0)

    def which(side):
        return 0 if side == 1 else 1

    firsts = {(half, side): slots(RING, "F1", half, side) for half in range(2) for side in SIDES}

    def send_first(half, j):
        for side in SIDES:
            rows = sum_rows(sum_block(half, 2, j), part_start(half, side), PART)
            send_in_loop(
                firsts[half, side] + j, part.at[rows, :], first1.at[half, which(side), j], f_device(half, side)
            )

    def send_second(half, j):
        for side in SIDES:
            block = sum_block(half, side, j)
            rows = sum_rows(block, part_start(half, side), PART)
            arrived(firsts[half, side] + j, first1.at[half, which(side), j])
            add_into(part, rows, [first1[half, which(side), j]])
        for side in SIDES:
            block = sum_block(half, side, j)
            rows = sum_rows(block, half * HALF, HALF)
            send(slot("F2", half, j, side), part.at[rows, :], first2.at[half, which(side), j], f_device(half, side))

    def take_second(half, j):
        for side in SIDES:
            arrived(slot("F2", half, j, side), first2.at[half, which(side), j])
        rows = sum_rows(sum_block(half, 0, j), half * HALF, HALF)
        add_into(part, rows, [first2[half, 0, j], first2[half, 1, j]])

    finish(block_at(2, 2))
    for half in range(2):
        send_first(half, 2)

    def outer(n, carried):
        place = pick(n, (1, 3, 0))
        finish(block_at(2, place))
        finish(block_at(place, 2))
        for half in range(2):
            send_first(half, place)
        return carried

    lax.fori_loop(0, 3, outer, 0)
    for half in range(2):
        send_second(half, 2)
    loop(corners, finish)
    for j in (1, 3):
        for half in range(2):
            send_second(half, j)
    loop([(1, 0), (3, 0), (0, 1), (0, 3), (0, 0)], finish)

    ahead = (2, 1, 3, 0)

    def weight_parts(n):
        first = wrap(y + ahead[n]) * 2

        def step(i, carried):
            chunk = first + jnp.where(i == 0, 1 - core, core)
            columns = pl.ds(pl.multiple_of(chunk * head, head), head)
            wg[chunk] = t_dot(xall[:, columns], g[...]).astype(BF16)
            return carried

        lax.fori_loop(0, 2, step, 0)
        send(slot("pair", n), wg.at[first + 1 - core], pair1.at[n], partner)

    def add_pair(n):
        chunk = wrap(y + ahead[n]) * 2 + core
        arrived(slot("pair", n), pair1.at[n])
        wg[chunk] = (wg[chunk].astype(F32) + pair1[n].astype(F32)).astype(BF16)

    weight_parts(0)
    for half in range(2):
        take_second(half, 2)
    for half in range(2):
        for side in SIDES:
            rows = sum_rows(sum_block(half, 0, 2), part_start(half, side), PART)
            send(slot("G1", half, side), part.at[rows, :], second1.at[half, which(side)], g_device(half, side))
    for half in range(2):
        send_second(half, 0)

    weight_parts(1)
    weight_parts(2)
    add_pair(0)
    for side in SIDES:
        chunk = wrap(y + 2) * 2 + core
        rows = pl.ds(0 if side == 1 else BLOCK, BLOCK)
        send(slot("Y1", side), wg.at[chunk, rows, :], ring1.at[which(side)], along_y(side))
    add_pair(1)
    weight_parts(3)
    add_pair(2)
    for side in SIDES:
        chunk = wrap(y + side) * 2 + core
        rows = pl.ds(0 if side == 1 else BLOCK, BLOCK)
        arrived(slot("Y1", side), ring1.at[which(side)])
        wg[chunk, rows, :] = (wg[chunk, rows, :].astype(F32) + ring1[which(side)].astype(F32)).astype(BF16)
        send(slot("Y2", side), wg.at[chunk], ring2.at[which(side)], along_y(side))
    add_pair(3)

    for j in (1, 3):
        for half in range(2):
            take_second(half, j)
    for half in range(2):
        for side in SIDES:
            block = sum_block(half, 0, side)
            arrived(slot("G1", half, side), second1.at[half, which(side)])
            add_into(part, sum_rows(block, part_start(half, side), PART), [second1[half, which(side)]])
            rows = sum_rows(block, half * HALF, HALF)
            send(slot("G2", half, side), part.at[rows, :], second2.at[half, which(side)], g_device(half, side))

    for half in range(2):
        take_second(half, 0)

    for side in SIDES:
        arrived(slot("Y2", side), ring2.at[which(side)])
    done_w[...] = wg[y * 2 + core].astype(F32) + ring2[0].astype(F32) + ring2[1].astype(F32)
    leave_w = pltpu.make_async_copy(done_w, out_w, local_sem.at[6])
    leave_w.start()

    for half in range(2):
        for side in SIDES:
            arrived(slot("G2", half, side), second2.at[half, which(side)])
        rows = sum_rows(sp, half * HALF, HALF)
        total = part[rows, :].astype(F32) + second2[half, 0].astype(F32) + second2[half, 1].astype(F32)
        done_x[half * HALF : (half + 1) * HALF, :] = total.astype(BF16)
    leave_x = pltpu.make_async_copy(done_x, out_x.at[0], local_sem.at[7])
    leave_x.start()
    leave_w.wait()
    leave_x.wait()

    for half in range(2):
        for side in SIDES:
            for j in range(RING):
                source = first1.at[half, which(side), j]
                copy(firsts[half, side] + j, source, source, partner).wait_send()
    for index, source in sent:
        copy(index, source, source, partner).wait_send()


A2A_ORDER = (1, 15, 4, 12, 3, 5, 11, 13, 2, 14, 8, 6, 7, 9, 10)
COPIES = 160
LATER = 1
VMEM_LIMIT = 67043328


def split_kernel(sum_x, sum_w, out_x, out_q, out_k, out_v, held_x, held_w, thirds, sems):
    head = out_q.shape[1]
    load_w = pltpu.make_async_copy(sum_w, held_w, sems.at[0])
    load_x = pltpu.make_async_copy(sum_x, held_x, sems.at[1])
    load_w.start()
    load_x.start()
    load_x.wait()
    leave_x = pltpu.make_async_copy(held_x, out_x, sems.at[2])
    leave_x.start()
    load_w.wait()
    leaves = [leave_x]
    for place, out in enumerate((out_q, out_k, out_v)):
        thirds[place] = held_w[:, place * head : (place + 1) * head] * (1.0 / (2 * RING))
        leave = pltpu.make_async_copy(thirds.at[place], out, sems.at[3 + place])
        leave.start()
        leaves.append(leave)
    for leave in leaves:
        leave.wait()


def body(hidden_in, mix_cotangent, query_weight, key_weight, value_weight, decay_log):
    depth = hidden_in.shape[2]
    head = query_weight.shape[1]
    blocks = RING * RING
    length = blocks * BLOCK
    wide = 3 * head
    anywhere = pl.BlockSpec(memory_space=pl.ANY)
    sum_x, sum_w = pl.pallas_call(
        all_kernel,
        out_shape=(
            jax.ShapeDtypeStruct(hidden_in.shape, BF16),
            jax.ShapeDtypeStruct((head, wide), F32),
        ),
        in_specs=[pl.BlockSpec(memory_space=pltpu.HBM)] + [anywhere] * 5,
        out_specs=(anywhere,) * 2,
        scratch_shapes=[
            pltpu.VMEM((length, depth), BF16),
            pltpu.VMEM((depth, wide), BF16),
            pltpu.VMEM((length, wide), BF16),
            pltpu.VMEM((length, head), BF16),
            pltpu.VMEM((length, wide), F32),
            pltpu.VMEM((BLOCK, BLOCK), F32),
            pltpu.VMEM((BLOCK, BLOCK), F32),
            pltpu.VMEM((BLOCK, head), F32),
            pltpu.VMEM((BLOCK, head), F32),
            pltpu.VMEM((blocks, head, head), F32),
            pltpu.VMEM((blocks, head, head), F32),
            pltpu.VMEM((blocks, head, head), BF16),
            pltpu.VMEM((blocks, head, head), BF16),
            pltpu.VMEM((length, wide), BF16),
            pltpu.VMEM((length, depth), BF16),
            pltpu.VMEM((2, 2, RING, PART, depth), BF16),
            pltpu.VMEM((2, 2, RING, HALF, depth), BF16),
            pltpu.VMEM((2, 2, PART, depth), BF16),
            pltpu.VMEM((2, 2, HALF, depth), BF16),
            pltpu.VMEM((2 * RING, depth // (2 * RING), wide), BF16),
            pltpu.VMEM((RING, depth // (2 * RING), wide), BF16),
            pltpu.VMEM((2, depth // (4 * RING), wide), BF16),
            pltpu.VMEM((2, depth // (2 * RING), wide), BF16),
            pltpu.SemaphoreType.DMA((8,)),
            pltpu.SemaphoreType.DMA((COPIES,)),
            pltpu.SemaphoreType.DMA((COPIES,)),
            pltpu.SemaphoreType.REGULAR((4,)),
            pltpu.SMEM((1,), F32),
            pltpu.VMEM((BLOCK, depth), BF16),
            pltpu.VMEM((head, wide), F32),
        ],
        compiler_params=pltpu.CompilerParams(
            vmem_limit_bytes=VMEM_LIMIT, collective_id=0, has_side_effects=True
        ),
        cost_estimate=pl.CostEstimate(flops=21 * 10**9, bytes_accessed=4 * 10**6, transcendentals=0),
    )(decay_log, hidden_in, mix_cotangent, query_weight, key_weight, value_weight)
    return pl.pallas_call(
        split_kernel,
        out_shape=(
            jax.ShapeDtypeStruct(hidden_in.shape, BF16),
            jax.ShapeDtypeStruct((head, head), F32),
            jax.ShapeDtypeStruct((head, head), F32),
            jax.ShapeDtypeStruct((head, head), F32),
        ),
        in_specs=[anywhere] * 2,
        out_specs=(anywhere,) * 4,
        scratch_shapes=[
            pltpu.VMEM(hidden_in.shape, BF16),
            pltpu.VMEM((head, wide), F32),
            pltpu.VMEM((3, head, head), F32),
            pltpu.SemaphoreType.DMA((6,)),
        ],
    )(sum_x, sum_w)


def solution(mesh):
    placed = (P("dp", "sp", None), P("dp", "sp", None), P("dp", "sp"), P("dp", "sp"), P("dp", "sp"), P("sp"))
    return jax.shard_map(
        body,
        mesh=mesh,
        in_specs=placed,
        out_specs=(P("dp", "sp", None), P("dp", "sp"), P("dp", "sp"), P("dp", "sp")),
        check_vma=False,
    )
```

```python
import jax
import jax.numpy as jnp
from jax import lax
from jax.experimental import pallas as pl
from jax.experimental.pallas import tpu as pltpu
from jax.sharding import PartitionSpec as P

BLOCK = 128
HALF = 64
PART = 32
RING = 4
F32 = jnp.float32
BF16 = jnp.bfloat16
MESH = pl.DeviceIdType.MESH
SIDES = (1, -1)


def dot(a, b):
    return lax.dot_general(a, b, (((1,), (0,)), ((), ())), preferred_element_type=F32)


def dot_t(a, b):
    return lax.dot_general(a, b, (((1,), (1,)), ((), ())), preferred_element_type=F32)


def t_dot(a, b):
    return lax.dot_general(a, b, (((0,), (0,)), ((), ())), preferred_element_type=F32)


def rows_of(block):
    return pl.ds(pl.multiple_of(block * BLOCK, BLOCK), BLOCK)


def pick(index, values):
    got = jnp.int32(values[-1])
    for place, value in enumerate(values[:-1]):
        got = jnp.where(index == place, jnp.int32(value), got)
    return got


def add_into(target, rows, others):
    total = target[rows, :].astype(F32)
    for other in others:
        total = total + other.astype(F32)
    target[rows, :] = total.astype(BF16)


def make_decays(rate, inner_ref, inner_t_ref, query_ref, key_ref):
    row = lax.broadcasted_iota(jnp.int32, (BLOCK, BLOCK), 0)
    col = lax.broadcasted_iota(jnp.int32, (BLOCK, BLOCK), 1)
    spread = (row - col).astype(F32)
    inner_ref[...] = jnp.where(spread >= 0, jnp.exp(rate * jnp.maximum(spread, 0.0)), 0.0)
    inner_t_ref[...] = jnp.where(spread <= 0, jnp.exp(rate * jnp.maximum(-spread, 0.0)), 0.0)
    offset = lax.broadcasted_iota(jnp.int32, query_ref.shape, 0).astype(F32)
    query_ref[...] = jnp.exp(rate * (offset + 1.0))
    key_ref[...] = jnp.exp(rate * (BLOCK - 1.0 - offset))


def in_block(block, head, scale, qkv, cot, decays, grads, fwd_states, bwd_states):
    inner_ref, inner_t_ref, query_ref, key_ref = decays
    rows = rows_of(block)
    queries = qkv[rows, 0:head]
    keys = qkv[rows, head : 2 * head]
    values = qkv[rows, 2 * head : 3 * head]
    given = cot[rows, :]
    mixed = (dot_t(given, values) * inner_ref[...]).astype(BF16)
    grads[rows, 0:head] = dot(mixed, keys)
    mixed_t = (dot_t(values, given) * inner_t_ref[...]).astype(BF16)
    grads[rows, head : 2 * head] = dot(mixed_t, queries) * scale
    scores_t = (dot_t(keys, queries) * inner_t_ref[...]).astype(BF16)
    grads[rows, 2 * head : 3 * head] = dot(scores_t, given)
    keys_w = (keys.astype(F32) * key_ref[...]).astype(BF16)
    fwd_states[block] = t_dot(keys_w, values)
    queries_w = (queries.astype(F32) * query_ref[...]).astype(BF16)
    bwd_states[block] = t_dot(queries_w, given)


def run_states(rate, blocks, fwd_states, bwd_states, fwd_bf, bwd_bf):
    size = 32
    wide = fwd_states.shape[2]
    step = jnp.exp(jnp.full((size, wide), BLOCK, F32) * rate)

    def chunk(n, carried):
        rows = pl.ds(pl.multiple_of(n * size, size), size)
        ahead = jnp.zeros((size, wide), F32)
        back = jnp.zeros((size, wide), F32)
        for i in range(blocks):
            fwd_bf[i, rows, :] = ahead.astype(BF16)
            ahead = ahead * step + fwd_states[i, rows, :]
            last = blocks - 1 - i
            bwd_bf[last, rows, :] = back.astype(BF16)
            back = back * step + bwd_states[last, rows, :]
        return carried

    lax.fori_loop(0, fwd_states.shape[1] // size, chunk, 0)


def cross_block(block, head, scale, qkv, cot, decays, grads, fwd_bf, bwd_bf, out):
    _, _, query_ref, key_ref = decays
    rows = rows_of(block)
    keys = qkv[rows, head : 2 * head]
    values = qkv[rows, 2 * head : 3 * head]
    state = fwd_bf[block]
    back = bwd_bf[block]
    grad_q = grads[rows, 0:head] + dot_t(cot[rows, :], state) * query_ref[...]
    grad_k = grads[rows, head : 2 * head] + dot_t(values, back) * (key_ref[...] * scale)
    grad_v = grads[rows, 2 * head : 3 * head] + dot(keys, back) * key_ref[...]
    out[rows, 0:head] = grad_q.astype(BF16)
    out[rows, head : 2 * head] = grad_k.astype(BF16)
    out[rows, 2 * head : 3 * head] = grad_v.astype(BF16)


def all_kernel(
    rate_ref,
    own_x,
    own_cot,
    wq_ref,
    wk_ref,
    wv_ref,
    out_x,
    out_w,
    xall,
    w,
    qkv,
    cot,
    grads,
    inner,
    inner_t,
    query_d,
    key_d,
    fwd,
    bwd,
    fwd_bf,
    bwd_bf,
    part,
    first1,
    first2,
    second1,
    second2,
    wg,
    pair1,
    ring1,
    ring2,
    local_sem,
    send_sem,
    recv_sem,
    ready_sem,
    rate_smem,
    done_x,
    done_w,
    wt,
):
    depth = xall.shape[1]
    head = cot.shape[1]
    blocks = RING * RING
    scale = head ** (-0.5)
    sp = lax.axis_index("sp")
    dp = lax.axis_index("dp")
    z, x = lax.div(sp, RING), lax.rem(sp, RING)
    y, core = lax.div(dp, 2), lax.rem(dp, 2)
    decays = (inner, inner_t, query_d, key_d)
    names = {}
    sent = []

    def slot(*name):
        return names.setdefault(name, len(names))

    def slots(count, *name):
        first = slot(*name, 0)
        for place in range(1, count):
            assert slot(*name, place) == first + place
        return first

    def wrap(value):
        return lax.rem(value + RING, RING)

    def block_at(dz, dx):
        return wrap(z + dz) * RING + wrap(x + dx)

    def plane(dz, dx):
        return (block_at(dz, dx), dp)

    def along_y(dy):
        return (sp, wrap(y + dy) * 2 + core)

    partner = (sp, y * 2 + 1 - core)

    def along(half, first, second):
        return (second, first) if half == 0 else (first, second)

    def copy(index, source, target, device):
        return pltpu.make_async_remote_copy(
            src_ref=source,
            dst_ref=target,
            send_sem=send_sem.at[index],
            recv_sem=recv_sem.at[index],
            device_id=device,
            device_id_type=MESH,
        )

    def send(index, source, target, device):
        copy(index, source, target, device).start()
        sent.append((index, source))

    def send_in_loop(index, source, target, device):
        copy(index, source, target, device).start()

    def arrived(index, target):
        copy(index, target, target, partner).wait_recv()

    barrier = pltpu.get_barrier_semaphore()
    beside = [plane(0, 1), plane(0, -1), plane(1, 0), plane(-1, 0)]
    friends = beside + [along_y(1), along_y(-1), partner]
    for friend in friends:
        pl.semaphore_signal(barrier, inc=1, device_id=friend, device_id_type=MESH)

    own_rows = rows_of(sp)
    w_rows = pl.ds(pl.multiple_of(dp * head, head), head)
    loads = [
        pltpu.make_async_copy(own_x.at[0], xall.at[own_rows, :], local_sem.at[0]),
        pltpu.make_async_copy(wq_ref, w.at[w_rows, 0:head], local_sem.at[1]),
        pltpu.make_async_copy(wk_ref, w.at[w_rows, head : 2 * head], local_sem.at[2]),
        pltpu.make_async_copy(wv_ref, w.at[w_rows, 2 * head : 3 * head], local_sem.at[3]),
        pltpu.make_async_copy(
            own_cot.at[0, :, pl.ds(pl.multiple_of(sp * head, head), head)], cot.at[own_rows, :], local_sem.at[4]
        ),
    ]
    loads.append(pltpu.make_async_copy(rate_ref, rate_smem, local_sem.at[5]))
    for load in loads:
        load.start()
    for load in loads:
        load.wait()
    rate = rate_smem[0]
    pl.semaphore_wait(barrier, len(friends))

    def x_rows(block, start, count):
        return xall.at[pl.ds(pl.multiple_of(block * BLOCK + start, PART), count), :]

    def part_start(half, side):
        return half * HALF + (0 if side == 1 else PART)

    def gather_block(half, p, q):
        return block_at(*along(half, p, q))

    def gather_send(name, half, p, q, side, axis):
        block = gather_block(half, p, q)
        if name[0] in ("s1", "s2"):
            rows = x_rows(block, half * HALF, HALF)
        else:
            rows = x_rows(block, part_start(half, side), PART)
        device = plane(*along(half, side, 0)) if axis == 0 else plane(*along(half, 0, side))
        send(slot(*name), rows, rows, device)

    def gather_wait(name, half, p, q, side):
        block = gather_block(half, p, q)
        if name[0] in ("s1", "s2"):
            rows = x_rows(block, half * HALF, HALF)
        else:
            rows = x_rows(block, part_start(half, side), PART)
        arrived(slot(*name), rows)

    def w_part(dy, which, start, count):
        first = (wrap(y + dy) * 2 + which) * head
        return w.at[pl.ds(pl.multiple_of(first + start, BLOCK), count), :]

    for side in SIDES:
        send(slot("w1", side), w_part(0, core, 0, head), w_part(0, core, 0, head), along_y(side))
    send(slot("wc", 0), w_part(0, core, 0, head), w_part(0, core, 0, head), partner)

    @pl.when(core == LATER)
    def _():
        pl.semaphore_wait(ready_sem.at[3], 1)

    for half in range(2):
        for side in SIDES:
            gather_send(("s1", half, side), half, 0, 0, side, 0)
    for half in range(2):
        for side in SIDES:
            gather_send(("s2", half, 0, side), half, 0, 0, side, 1)
    for turn in range(3):
        for friend in beside:
            pl.semaphore_signal(ready_sem.at[turn], inc=1, device_id=friend, device_id_type=MESH)
        pl.semaphore_wait(ready_sem.at[turn], len(beside))
    for offset in A2A_ORDER:
        target = lax.rem(sp + offset, blocks)
        send(
            slot("cot", offset),
            own_cot.at[0, :, pl.ds(pl.multiple_of(target * head, head), head)],
            cot.at[own_rows, :],
            (target, dp),
        )

    make_decays(rate, *decays)

    def project(block):
        rows = rows_of(block)
        got = dot(xall[rows, :], w[...])
        qkv[rows, 0:head] = got[:, 0:head].astype(BF16)
        qkv[rows, head : 2 * head] = (got[:, head : 2 * head].astype(BF16).astype(F32) * scale).astype(BF16)
        qkv[rows, 2 * head : 3 * head] = got[:, 2 * head : 3 * head].astype(BF16)

    def inside(block):
        in_block(block, head, scale, qkv, cot, decays, grads, fwd, bwd)

    def loop(places, *works):
        several = 2 if len(places) % 2 == 0 else 1

        def step(n, carried):
            group = []
            for m in range(several):
                at = n * several + m
                group.append(block_at(pick(at, [dz for dz, _ in places]), pick(at, [dx for _, dx in places])))
            for work in works:
                for block in group:
                    work(block)
            return carried

        lax.fori_loop(0, len(places) // several, step, 0)

    near = [(0, 0), (0, 1), (0, 3), (1, 0), (3, 0)]
    corners = [(1, 1), (1, 3), (3, 1), (3, 3)]
    far = [(0, 2), (2, 0)]
    last = [(2, 2)]

    for half in range(2):
        for side in SIDES:
            gather_wait(("s1", half, side), half, -side, 0, side)
            gather_send(("f1", half, side), half, -side, 0, side, 0)
    for half in range(2):
        for near_p in SIDES:
            for side in SIDES:
                gather_send(("s2", half, near_p, side), half, near_p, 0, side, 1)

    for side in SIDES:
        arrived(slot("w1", side), w_part(-side, core, 0, head))
        rows = w_part(-side, core, 0 if side == 1 else BLOCK, BLOCK)
        send(slot("w2", side), rows, rows, along_y(side))
        rows = w_part(-side, core, 0, head)
        send(slot("wc", side), rows, rows, partner)

    @pl.when(core != LATER)
    def _():
        pl.semaphore_signal(ready_sem.at[3], inc=1, device_id=partner, device_id_type=MESH)

    for half in range(2):
        for side in SIDES:
            gather_wait(("s2", half, 0, side), half, 0, -side, side)
            gather_send(("f2", half, 0, side), half, 0, -side, side, 1)

    for side in SIDES:
        arrived(slot("w2", side), w_part(2, core, 0 if side == 1 else BLOCK, BLOCK))
    send(slot("wc", 2), w_part(2, core, 0, head), w_part(2, core, 0, head), partner)
    for dy in (0, 1, -1, 2):
        arrived(slot("wc", dy), w_part(-dy, 1 - core, 0, head))

    loop(near, project)

    def turn_weights(n, carried):
        rows = pl.ds(pl.multiple_of(n * head, head), head)
        for third in range(3):
            wt[third * head : (third + 1) * head, rows] = w[rows, third * head : (third + 1) * head].T
        return carried

    lax.fori_loop(0, depth // head, turn_weights, 0)

    for half in range(2):
        for side in SIDES:
            gather_wait(("f1", half, side), half, 2, 0, side)
    for half in range(2):
        for side in SIDES:
            gather_send(("s2", half, 2, side), half, 2, 0, side, 1)

    for offset in A2A_ORDER:
        arrived(slot("cot", offset), cot.at[rows_of(lax.rem(sp + blocks - offset, blocks)), :])
    loop(near, inside)

    for near_p in SIDES:
        for half in range(2):
            for side in SIDES:
                gather_wait(("s2", half, near_p, side), half, near_p, -side, side)
                gather_send(("f2", half, near_p, side), half, near_p, -side, side, 1)
    loop(corners, project, inside)

    for half in range(2):
        for side in SIDES:
            gather_wait(("f2", half, 0, side), half, 0, 2, side)
    loop(far, project, inside)

    for half in range(2):
        for side in SIDES:
            gather_wait(("s2", half, 2, side), half, 2, -side, side)
            gather_send(("f2", half, 2, side), half, 2, -side, side, 1)

    for near_p in SIDES:
        for half in range(2):
            for side in SIDES:
                gather_wait(("f2", half, near_p, side), half, near_p, 2, side)
        loop([(2, near_p), (near_p, 2)], project, inside)

    for half in range(2):
        for side in SIDES:
            gather_wait(("f2", half, 2, side), half, 2, 2, side)
    loop(last, project, inside)

    run_states(rate, blocks, fwd, bwd, fwd_bf, bwd_bf)

    def finish_all(group):
        for block in group:
            cross_block(block, head, scale, qkv, cot, decays, grads, fwd_bf, bwd_bf, qkv)
        got = jnp.concatenate([qkv[rows_of(block), :] for block in group], axis=0)
        sums = dot(got, wt[...]).astype(BF16)
        for place, block in enumerate(group):
            part[rows_of(block), :] = sums[place * BLOCK : (place + 1) * BLOCK, :]

    def finish_loop(places):
        def step(n, carried):
            group = []
            for m in range(2):
                at = n * 2 + m
                group.append(block_at(pick(at, [dz for dz, _ in places]), pick(at, [dx for _, dx in places])))
            finish_all(group)
            return carried

        lax.fori_loop(0, len(places) // 2, step, 0)

    def sum_block(half, f, q):
        return block_at(*((f, q) if half == 0 else (q, f)))

    def sum_rows(block, start, count):
        return pl.ds(pl.multiple_of(block * BLOCK + start, PART), count)

    def f_device(half, side):
        return plane(side, 0) if half == 0 else plane(0, side)

    def g_device(half, side):
        return plane(0, side) if half == 0 else plane(side, 0)

    def which(side):
        return 0 if side == 1 else 1

    firsts = {(half, side): slots(RING, "F1", half, side) for half in range(2) for side in SIDES}

    def send_first(half, j):
        for side in SIDES:
            rows = sum_rows(sum_block(half, 2, j), part_start(half, side), PART)
            send_in_loop(
                firsts[half, side] + j, part.at[rows, :], first1.at[half, which(side), j], f_device(half, side)
            )

    def send_second(half, j):
        for side in SIDES:
            block = sum_block(half, side, j)
            rows = sum_rows(block, part_start(half, side), PART)
            arrived(firsts[half, side] + j, first1.at[half, which(side), j])
            add_into(part, rows, [first1[half, which(side), j]])
        for side in SIDES:
            block = sum_block(half, side, j)
            rows = sum_rows(block, half * HALF, HALF)
            send(slot("F2", half, j, side), part.at[rows, :], first2.at[half, which(side), j], f_device(half, side))

    def take_second(half, j):
        for side in SIDES:
            arrived(slot("F2", half, j, side), first2.at[half, which(side), j])
        rows = sum_rows(sum_block(half, 0, j), half * HALF, HALF)
        add_into(part, rows, [first2[half, 0, j], first2[half, 1, j]])

    finish_all([block_at(2, 2)])
    for half in range(2):
        send_first(half, 2)

    def outer(n, carried):
        place = pick(n, (1, 3, 0))
        finish_all([block_at(2, place), block_at(place, 2)])
        for half in range(2):
            send_first(half, place)
        return carried

    lax.fori_loop(0, 3, outer, 0)
    for half in range(2):
        send_second(half, 2)
    finish_loop(corners)
    for j in (1, 3):
        for half in range(2):
            send_second(half, j)
    finish_loop([(1, 0), (3, 0), (0, 1), (0, 3)])
    finish_all([block_at(0, 0)])

    ahead = (2, 1, 3, 0)

    def weight_parts(n):
        first = wrap(y + ahead[n]) * 2

        def step(i, carried):
            chunk = first + jnp.where(i == 0, 1 - core, core)
            columns = pl.ds(pl.multiple_of(chunk * head, head), head)
            wg[chunk] = t_dot(xall[:, columns], qkv[...]).astype(BF16)
            return carried

        lax.fori_loop(0, 2, step, 0)
        send(slot("pair", n), wg.at[first + 1 - core], pair1.at[n], partner)

    def add_pair(n):
        chunk = wrap(y + ahead[n]) * 2 + core
        arrived(slot("pair", n), pair1.at[n])
        wg[chunk] = (wg[chunk].astype(F32) + pair1[n].astype(F32)).astype(BF16)

    weight_parts(0)
    for half in range(2):
        take_second(half, 2)
    for half in range(2):
        for side in SIDES:
            rows = sum_rows(sum_block(half, 0, 2), part_start(half, side), PART)
            send(slot("G1", half, side), part.at[rows, :], second1.at[half, which(side)], g_device(half, side))
    for half in range(2):
        send_second(half, 0)

    weight_parts(1)
    weight_parts(2)
    add_pair(0)
    for side in SIDES:
        chunk = wrap(y + 2) * 2 + core
        rows = pl.ds(0 if side == 1 else BLOCK, BLOCK)
        send(slot("Y1", side), wg.at[chunk, rows, :], ring1.at[which(side)], along_y(side))
    add_pair(1)
    weight_parts(3)
    add_pair(2)
    for side in SIDES:
        chunk = wrap(y + side) * 2 + core
        rows = pl.ds(0 if side == 1 else BLOCK, BLOCK)
        arrived(slot("Y1", side), ring1.at[which(side)])
        wg[chunk, rows, :] = (wg[chunk, rows, :].astype(F32) + ring1[which(side)].astype(F32)).astype(BF16)
        send(slot("Y2", side), wg.at[chunk], ring2.at[which(side)], along_y(side))
    add_pair(3)

    for j in (1, 3):
        for half in range(2):
            take_second(half, j)
    for half in range(2):
        for side in SIDES:
            block = sum_block(half, 0, side)
            arrived(slot("G1", half, side), second1.at[half, which(side)])
            add_into(part, sum_rows(block, part_start(half, side), PART), [second1[half, which(side)]])
            rows = sum_rows(block, half * HALF, HALF)
            send(slot("G2", half, side), part.at[rows, :], second2.at[half, which(side)], g_device(half, side))

    for half in range(2):
        take_second(half, 0)

    for side in SIDES:
        arrived(slot("Y2", side), ring2.at[which(side)])
    done_w[...] = wg[y * 2 + core].astype(F32) + ring2[0].astype(F32) + ring2[1].astype(F32)
    leave_w = pltpu.make_async_copy(done_w, out_w, local_sem.at[6])
    leave_w.start()

    for half in range(2):
        for side in SIDES:
            arrived(slot("G2", half, side), second2.at[half, which(side)])
        rows = sum_rows(sp, half * HALF, HALF)
        total = part[rows, :].astype(F32) + second2[half, 0].astype(F32) + second2[half, 1].astype(F32)
        done_x[half * HALF : (half + 1) * HALF, :] = total.astype(BF16)
    leave_x = pltpu.make_async_copy(done_x, out_x.at[0], local_sem.at[7])
    leave_x.start()
    leave_w.wait()
    leave_x.wait()

    for half in range(2):
        for side in SIDES:
            for j in range(RING):
                source = first1.at[half, which(side), j]
                copy(firsts[half, side] + j, source, source, partner).wait_send()
    for index, source in sent:
        copy(index, source, source, partner).wait_send()


A2A_ORDER = (1, 15, 4, 12, 3, 5, 11, 13, 2, 14, 8, 6, 7, 9, 10)
COPIES = 160
LATER = 1
VMEM_LIMIT = 67043328


def split_kernel(sum_x, sum_w, out_x, out_q, out_k, out_v, held_x, held_w, thirds, sems):
    head = out_q.shape[1]
    load_w = pltpu.make_async_copy(sum_w, held_w, sems.at[0])
    load_x = pltpu.make_async_copy(sum_x, held_x, sems.at[1])
    load_w.start()
    load_x.start()
    load_x.wait()
    leave_x = pltpu.make_async_copy(held_x, out_x, sems.at[2])
    leave_x.start()
    load_w.wait()
    leaves = [leave_x]
    for place, out in enumerate((out_q, out_k, out_v)):
        thirds[place] = held_w[:, place * head : (place + 1) * head] * (1.0 / (2 * RING))
        leave = pltpu.make_async_copy(thirds.at[place], out, sems.at[3 + place])
        leave.start()
        leaves.append(leave)
    for leave in leaves:
        leave.wait()


def body(hidden_in, mix_cotangent, query_weight, key_weight, value_weight, decay_log):
    depth = hidden_in.shape[2]
    head = query_weight.shape[1]
    blocks = RING * RING
    length = blocks * BLOCK
    wide = 3 * head
    anywhere = pl.BlockSpec(memory_space=pl.ANY)
    sum_x, sum_w = pl.pallas_call(
        all_kernel,
        out_shape=(
            jax.ShapeDtypeStruct(hidden_in.shape, BF16),
            jax.ShapeDtypeStruct((head, wide), F32),
        ),
        in_specs=[pl.BlockSpec(memory_space=pltpu.HBM)] + [anywhere] * 5,
        out_specs=(anywhere,) * 2,
        scratch_shapes=[
            pltpu.VMEM((length, depth), BF16),
            pltpu.VMEM((depth, wide), BF16),
            pltpu.VMEM((length, wide), BF16),
            pltpu.VMEM((length, head), BF16),
            pltpu.VMEM((length, wide), F32),
            pltpu.VMEM((BLOCK, BLOCK), F32),
            pltpu.VMEM((BLOCK, BLOCK), F32),
            pltpu.VMEM((BLOCK, head), F32),
            pltpu.VMEM((BLOCK, head), F32),
            pltpu.VMEM((blocks, head, head), F32),
            pltpu.VMEM((blocks, head, head), F32),
            pltpu.VMEM((blocks, head, head), BF16),
            pltpu.VMEM((blocks, head, head), BF16),
            pltpu.VMEM((length, depth), BF16),
            pltpu.VMEM((2, 2, RING, PART, depth), BF16),
            pltpu.VMEM((2, 2, RING, HALF, depth), BF16),
            pltpu.VMEM((2, 2, PART, depth), BF16),
            pltpu.VMEM((2, 2, HALF, depth), BF16),
            pltpu.VMEM((2 * RING, depth // (2 * RING), wide), BF16),
            pltpu.VMEM((RING, depth // (2 * RING), wide), BF16),
            pltpu.VMEM((2, depth // (4 * RING), wide), BF16),
            pltpu.VMEM((2, depth // (2 * RING), wide), BF16),
            pltpu.SemaphoreType.DMA((8,)),
            pltpu.SemaphoreType.DMA((COPIES,)),
            pltpu.SemaphoreType.DMA((COPIES,)),
            pltpu.SemaphoreType.REGULAR((4,)),
            pltpu.SMEM((1,), F32),
            pltpu.VMEM((BLOCK, depth), BF16),
            pltpu.VMEM((head, wide), F32),
            pltpu.VMEM((wide, depth), BF16),
        ],
        compiler_params=pltpu.CompilerParams(
            vmem_limit_bytes=VMEM_LIMIT, collective_id=0, has_side_effects=True
        ),
        cost_estimate=pl.CostEstimate(flops=21 * 10**9, bytes_accessed=4 * 10**6, transcendentals=0),
    )(decay_log, hidden_in, mix_cotangent, query_weight, key_weight, value_weight)
    return pl.pallas_call(
        split_kernel,
        out_shape=(
            jax.ShapeDtypeStruct(hidden_in.shape, BF16),
            jax.ShapeDtypeStruct((head, head), F32),
            jax.ShapeDtypeStruct((head, head), F32),
            jax.ShapeDtypeStruct((head, head), F32),
        ),
        in_specs=[anywhere] * 2,
        out_specs=(anywhere,) * 4,
        scratch_shapes=[
            pltpu.VMEM(hidden_in.shape, BF16),
            pltpu.VMEM((head, wide), F32),
            pltpu.VMEM((3, head, head), F32),
            pltpu.SemaphoreType.DMA((6,)),
        ],
    )(sum_x, sum_w)


def solution(mesh):
    placed = (P("dp", "sp", None), P("dp", "sp", None), P("dp", "sp"), P("dp", "sp"), P("dp", "sp"), P("sp"))
    return jax.shard_map(
        body,
        mesh=mesh,
        in_specs=placed,
        out_specs=(P("dp", "sp", None), P("dp", "sp"), P("dp", "sp"), P("dp", "sp")),
        check_vma=False,
    )
```

```python
import jax
import jax.numpy as jnp
from jax import lax
from jax.experimental import pallas as pl
from jax.experimental.pallas import tpu as pltpu
from jax.sharding import PartitionSpec as P

BLOCK = 128
HALF = 64
PART = 32
RING = 4
F32 = jnp.float32
BF16 = jnp.bfloat16
MESH = pl.DeviceIdType.MESH
SIDES = (1, -1)


def dot(a, b):
    return lax.dot_general(a, b, (((1,), (0,)), ((), ())), preferred_element_type=F32)


def dot_t(a, b):
    return lax.dot_general(a, b, (((1,), (1,)), ((), ())), preferred_element_type=F32)


def t_dot(a, b):
    return lax.dot_general(a, b, (((0,), (0,)), ((), ())), preferred_element_type=F32)


def rows_of(block):
    return pl.ds(pl.multiple_of(block * BLOCK, BLOCK), BLOCK)


def pick(index, values):
    got = jnp.int32(values[-1])
    for place, value in enumerate(values[:-1]):
        got = jnp.where(index == place, jnp.int32(value), got)
    return got


def add_into(target, rows, others):
    total = target[rows, :].astype(F32)
    for other in others:
        total = total + other.astype(F32)
    target[rows, :] = total.astype(BF16)


def make_decays(rate, inner_ref, inner_t_ref, query_ref, key_ref):
    row = lax.broadcasted_iota(jnp.int32, (BLOCK, BLOCK), 0)
    col = lax.broadcasted_iota(jnp.int32, (BLOCK, BLOCK), 1)
    spread = (row - col).astype(F32)
    inner_ref[...] = jnp.where(spread >= 0, jnp.exp(rate * jnp.maximum(spread, 0.0)), 0.0)
    inner_t_ref[...] = jnp.where(spread <= 0, jnp.exp(rate * jnp.maximum(-spread, 0.0)), 0.0)
    offset = lax.broadcasted_iota(jnp.int32, query_ref.shape, 0).astype(F32)
    query_ref[...] = jnp.exp(rate * (offset + 1.0))
    key_ref[...] = jnp.exp(rate * (BLOCK - 1.0 - offset))


def in_block(block, head, scale, qkv, cot, decays, grads, fwd_states, bwd_states):
    inner_ref, inner_t_ref, query_ref, key_ref = decays
    rows = rows_of(block)
    queries = qkv[rows, 0:head]
    keys = qkv[rows, head : 2 * head]
    values = qkv[rows, 2 * head : 3 * head]
    given = cot[rows, :]
    mixed = (dot_t(given, values) * inner_ref[...]).astype(BF16)
    grads[rows, 0:head] = dot(mixed, keys)
    mixed_t = (dot_t(values, given) * inner_t_ref[...]).astype(BF16)
    grads[rows, head : 2 * head] = dot(mixed_t, queries) * scale
    scores_t = (dot_t(keys, queries) * inner_t_ref[...]).astype(BF16)
    grads[rows, 2 * head : 3 * head] = dot(scores_t, given)
    keys_w = (keys.astype(F32) * key_ref[...]).astype(BF16)
    fwd_states[block] = t_dot(keys_w, values)
    queries_w = (queries.astype(F32) * query_ref[...]).astype(BF16)
    bwd_states[block] = t_dot(queries_w, given)


def run_states(rate, blocks, fwd_states, bwd_states, fwd_bf, bwd_bf):
    size = 32
    wide = fwd_states.shape[2]
    step = jnp.exp(jnp.full((size, wide), BLOCK, F32) * rate)

    def chunk(n, carried):
        rows = pl.ds(pl.multiple_of(n * size, size), size)
        ahead = jnp.zeros((size, wide), F32)
        back = jnp.zeros((size, wide), F32)
        for i in range(blocks):
            fwd_bf[i, rows, :] = ahead.astype(BF16)
            ahead = ahead * step + fwd_states[i, rows, :]
            last = blocks - 1 - i
            bwd_bf[last, rows, :] = back.astype(BF16)
            back = back * step + bwd_states[last, rows, :]
        return carried

    lax.fori_loop(0, fwd_states.shape[1] // size, chunk, 0)


def cross_block(block, head, scale, qkv, cot, decays, grads, fwd_bf, bwd_bf, out):
    _, _, query_ref, key_ref = decays
    rows = rows_of(block)
    keys = qkv[rows, head : 2 * head]
    values = qkv[rows, 2 * head : 3 * head]
    state = fwd_bf[block]
    back = bwd_bf[block]
    grad_q = grads[rows, 0:head] + dot_t(cot[rows, :], state) * query_ref[...]
    grad_k = grads[rows, head : 2 * head] + dot_t(values, back) * (key_ref[...] * scale)
    grad_v = grads[rows, 2 * head : 3 * head] + dot(keys, back) * key_ref[...]
    out[rows, 0:head] = grad_q.astype(BF16)
    out[rows, head : 2 * head] = grad_k.astype(BF16)
    out[rows, 2 * head : 3 * head] = grad_v.astype(BF16)


def all_kernel(
    rate_ref,
    own_x,
    own_cot,
    wq_ref,
    wk_ref,
    wv_ref,
    out_x,
    out_w,
    xall,
    w,
    qkv,
    cot,
    grads,
    inner,
    inner_t,
    query_d,
    key_d,
    fwd,
    bwd,
    fwd_bf,
    bwd_bf,
    part,
    first1,
    first2,
    second1,
    second2,
    wg,
    pair1,
    ring1,
    ring2,
    local_sem,
    send_sem,
    recv_sem,
    ready_sem,
    rate_smem,
    done_x,
    done_w,
    wt,
):
    depth = xall.shape[1]
    head = cot.shape[1]
    blocks = RING * RING
    scale = head ** (-0.5)
    sp = lax.axis_index("sp")
    dp = lax.axis_index("dp")
    z, x = lax.div(sp, RING), lax.rem(sp, RING)
    y, core = lax.div(dp, 2), lax.rem(dp, 2)
    decays = (inner, inner_t, query_d, key_d)
    names = {}
    sent = []

    def slot(*name):
        return names.setdefault(name, len(names))

    def slots(count, *name):
        first = slot(*name, 0)
        for place in range(1, count):
            assert slot(*name, place) == first + place
        return first

    def wrap(value):
        return lax.rem(value + RING, RING)

    def block_at(dz, dx):
        return wrap(z + dz) * RING + wrap(x + dx)

    def plane(dz, dx):
        return (block_at(dz, dx), dp)

    def along_y(dy):
        return (sp, wrap(y + dy) * 2 + core)

    partner = (sp, y * 2 + 1 - core)

    def along(half, first, second):
        return (second, first) if half == 0 else (first, second)

    def copy(index, source, target, device):
        return pltpu.make_async_remote_copy(
            src_ref=source,
            dst_ref=target,
            send_sem=send_sem.at[index],
            recv_sem=recv_sem.at[index],
            device_id=device,
            device_id_type=MESH,
        )

    def send(index, source, target, device):
        copy(index, source, target, device).start()
        sent.append((index, source))

    def send_in_loop(index, source, target, device):
        copy(index, source, target, device).start()

    def arrived(index, target):
        copy(index, target, target, partner).wait_recv()

    barrier = pltpu.get_barrier_semaphore()
    beside = [plane(0, 1), plane(0, -1), plane(1, 0), plane(-1, 0)]
    friends = beside + [along_y(1), along_y(-1), partner]
    for friend in friends:
        pl.semaphore_signal(barrier, inc=1, device_id=friend, device_id_type=MESH)

    own_rows = rows_of(sp)
    w_rows = pl.ds(pl.multiple_of(dp * head, head), head)
    loads = [
        pltpu.make_async_copy(own_x.at[0], xall.at[own_rows, :], local_sem.at[0]),
        pltpu.make_async_copy(wq_ref, w.at[w_rows, 0:head], local_sem.at[1]),
        pltpu.make_async_copy(wk_ref, w.at[w_rows, head : 2 * head], local_sem.at[2]),
        pltpu.make_async_copy(wv_ref, w.at[w_rows, 2 * head : 3 * head], local_sem.at[3]),
        pltpu.make_async_copy(
            own_cot.at[0, :, pl.ds(pl.multiple_of(sp * head, head), head)], cot.at[own_rows, :], local_sem.at[4]
        ),
    ]
    loads.append(pltpu.make_async_copy(rate_ref, rate_smem, local_sem.at[5]))
    for load in loads:
        load.start()
    for load in loads:
        load.wait()
    rate = rate_smem[0]
    pl.semaphore_wait(barrier, len(friends))

    def x_rows(block, start, count):
        return xall.at[pl.ds(pl.multiple_of(block * BLOCK + start, PART), count), :]

    def part_start(half, side):
        return half * HALF + (0 if side == 1 else PART)

    def gather_block(half, p, q):
        return block_at(*along(half, p, q))

    def gather_send(name, half, p, q, side, axis):
        block = gather_block(half, p, q)
        if name[0] in ("s1", "s2"):
            rows = x_rows(block, half * HALF, HALF)
        else:
            rows = x_rows(block, part_start(half, side), PART)
        device = plane(*along(half, side, 0)) if axis == 0 else plane(*along(half, 0, side))
        send(slot(*name), rows, rows, device)

    def gather_wait(name, half, p, q, side):
        block = gather_block(half, p, q)
        if name[0] in ("s1", "s2"):
            rows = x_rows(block, half * HALF, HALF)
        else:
            rows = x_rows(block, part_start(half, side), PART)
        arrived(slot(*name), rows)

    def w_part(dy, which, start, count):
        first = (wrap(y + dy) * 2 + which) * head
        return w.at[pl.ds(pl.multiple_of(first + start, BLOCK), count), :]

    for side in SIDES:
        send(slot("w1", side), w_part(0, core, 0, head), w_part(0, core, 0, head), along_y(side))
    send(slot("wc", 0), w_part(0, core, 0, head), w_part(0, core, 0, head), partner)

    @pl.when(core == LATER)
    def _():
        pl.semaphore_wait(ready_sem.at[3], 1)

    for half in range(2):
        for side in SIDES:
            gather_send(("s1", half, side), half, 0, 0, side, 0)
    for half in range(2):
        for side in SIDES:
            gather_send(("s2", half, 0, side), half, 0, 0, side, 1)
    for turn in range(3):
        for friend in beside:
            pl.semaphore_signal(ready_sem.at[turn], inc=1, device_id=friend, device_id_type=MESH)
        pl.semaphore_wait(ready_sem.at[turn], len(beside))
    for offset in A2A_ORDER:
        target = lax.rem(sp + offset, blocks)
        send(
            slot("cot", offset),
            own_cot.at[0, :, pl.ds(pl.multiple_of(target * head, head), head)],
            cot.at[own_rows, :],
            (target, dp),
        )

    make_decays(rate, *decays)

    def project(block):
        rows = rows_of(block)
        got = dot(xall[rows, :], w[...])
        qkv[rows, 0:head] = got[:, 0:head].astype(BF16)
        qkv[rows, head : 2 * head] = (got[:, head : 2 * head].astype(BF16).astype(F32) * scale).astype(BF16)
        qkv[rows, 2 * head : 3 * head] = got[:, 2 * head : 3 * head].astype(BF16)

    def inside(block):
        in_block(block, head, scale, qkv, cot, decays, grads, fwd, bwd)

    def loop(places, *works):
        several = 2 if len(places) % 2 == 0 else 1

        def step(n, carried):
            group = []
            for m in range(several):
                at = n * several + m
                group.append(block_at(pick(at, [dz for dz, _ in places]), pick(at, [dx for _, dx in places])))
            for work in works:
                for block in group:
                    work(block)
            return carried

        lax.fori_loop(0, len(places) // several, step, 0)

    near = [(0, 0), (0, 1), (0, 3), (1, 0), (3, 0)]
    corners = [(1, 1), (1, 3), (3, 1), (3, 3)]
    far = [(0, 2), (2, 0)]
    last = [(2, 2)]

    for half in range(2):
        for side in SIDES:
            gather_wait(("s1", half, side), half, -side, 0, side)
            gather_send(("f1", half, side), half, -side, 0, side, 0)
    for half in range(2):
        for near_p in SIDES:
            for side in SIDES:
                gather_send(("s2", half, near_p, side), half, near_p, 0, side, 1)

    for side in SIDES:
        arrived(slot("w1", side), w_part(-side, core, 0, head))
        rows = w_part(-side, core, 0 if side == 1 else BLOCK, BLOCK)
        send(slot("w2", side), rows, rows, along_y(side))
        rows = w_part(-side, core, 0, head)
        send(slot("wc", side), rows, rows, partner)

    @pl.when(core != LATER)
    def _():
        pl.semaphore_signal(ready_sem.at[3], inc=1, device_id=partner, device_id_type=MESH)

    for half in range(2):
        for side in SIDES:
            gather_wait(("s2", half, 0, side), half, 0, -side, side)
            gather_send(("f2", half, 0, side), half, 0, -side, side, 1)

    for side in SIDES:
        arrived(slot("w2", side), w_part(2, core, 0 if side == 1 else BLOCK, BLOCK))
    send(slot("wc", 2), w_part(2, core, 0, head), w_part(2, core, 0, head), partner)
    for dy in (0, 1, -1, 2):
        arrived(slot("wc", dy), w_part(-dy, 1 - core, 0, head))

    loop(near, project)

    def turn_weights(n, carried):
        rows = pl.ds(pl.multiple_of(n * head, head), head)
        for third in range(3):
            wt[third * head : (third + 1) * head, rows] = w[rows, third * head : (third + 1) * head].T
        return carried

    lax.fori_loop(0, depth // head, turn_weights, 0)

    for half in range(2):
        for side in SIDES:
            gather_wait(("f1", half, side), half, 2, 0, side)
    for half in range(2):
        for side in SIDES:
            gather_send(("s2", half, 2, side), half, 2, 0, side, 1)

    for offset in A2A_ORDER:
        arrived(slot("cot", offset), cot.at[rows_of(lax.rem(sp + blocks - offset, blocks)), :])
    loop(near, inside)

    for near_p in SIDES:
        for half in range(2):
            for side in SIDES:
                gather_wait(("s2", half, near_p, side), half, near_p, -side, side)
                gather_send(("f2", half, near_p, side), half, near_p, -side, side, 1)
    loop(corners, project, inside)

    for half in range(2):
        for side in SIDES:
            gather_wait(("f2", half, 0, side), half, 0, 2, side)
    loop(far, project, inside)

    for half in range(2):
        for side in SIDES:
            gather_wait(("s2", half, 2, side), half, 2, -side, side)
            gather_send(("f2", half, 2, side), half, 2, -side, side, 1)

    for near_p in SIDES:
        for half in range(2):
            for side in SIDES:
                gather_wait(("f2", half, near_p, side), half, near_p, 2, side)
        loop([(2, near_p), (near_p, 2)], project, inside)

    for half in range(2):
        for side in SIDES:
            gather_wait(("f2", half, 2, side), half, 2, 2, side)
    loop(last, project, inside)

    run_states(rate, blocks, fwd, bwd, fwd_bf, bwd_bf)

    def finish_all(group):
        for block in group:
            cross_block(block, head, scale, qkv, cot, decays, grads, fwd_bf, bwd_bf, qkv)
        got = jnp.concatenate([qkv[rows_of(block), :] for block in group], axis=0)
        sums = dot(got, wt[...]).astype(BF16)
        for place, block in enumerate(group):
            part[rows_of(block), :] = sums[place * BLOCK : (place + 1) * BLOCK, :]

    def finish_loop(places):
        def step(n, carried):
            group = []
            for m in range(2):
                at = n * 2 + m
                group.append(block_at(pick(at, [dz for dz, _ in places]), pick(at, [dx for _, dx in places])))
            finish_all(group)
            return carried

        lax.fori_loop(0, len(places) // 2, step, 0)

    def sum_block(half, f, q):
        return block_at(*((f, q) if half == 0 else (q, f)))

    def sum_rows(block, start, count):
        return pl.ds(pl.multiple_of(block * BLOCK + start, PART), count)

    def f_device(half, side):
        return plane(side, 0) if half == 0 else plane(0, side)

    def g_device(half, side):
        return plane(0, side) if half == 0 else plane(side, 0)

    def which(side):
        return 0 if side == 1 else 1

    firsts = {(half, side): slots(RING, "F1", half, side) for half in range(2) for side in SIDES}

    def send_first(half, j):
        for side in SIDES:
            rows = sum_rows(sum_block(half, 2, j), part_start(half, side), PART)
            send_in_loop(
                firsts[half, side] + j, part.at[rows, :], first1.at[half, which(side), j], f_device(half, side)
            )

    def send_second(half, j):
        for side in SIDES:
            block = sum_block(half, side, j)
            rows = sum_rows(block, part_start(half, side), PART)
            arrived(firsts[half, side] + j, first1.at[half, which(side), j])
            add_into(part, rows, [first1[half, which(side), j]])
        for side in SIDES:
            block = sum_block(half, side, j)
            rows = sum_rows(block, half * HALF, HALF)
            send(slot("F2", half, j, side), part.at[rows, :], first2.at[half, which(side), j], f_device(half, side))

    def take_second(half, j):
        for side in SIDES:
            arrived(slot("F2", half, j, side), first2.at[half, which(side), j])
        rows = sum_rows(sum_block(half, 0, j), half * HALF, HALF)
        add_into(part, rows, [first2[half, 0, j], first2[half, 1, j]])

    finish_all([block_at(2, 2)])
    for half in range(2):
        send_first(half, 2)

    def outer(n, carried):
        place = pick(n, (1, 3, 0))
        finish_all([block_at(2, place), block_at(place, 2)])
        for half in range(2):
            send_first(half, place)
        return carried

    lax.fori_loop(0, 3, outer, 0)
    for half in range(2):
        send_second(half, 2)
    finish_loop(corners)
    for j in (1, 3):
        for half in range(2):
            send_second(half, j)
    finish_loop([(1, 0), (3, 0), (0, 1), (0, 3)])
    finish_all([block_at(0, 0)])

    ahead = (2, 1, 3, 0)

    def weight_parts(n):
        first = wrap(y + ahead[n]) * 2

        def step(i, carried):
            chunk = first + jnp.where(i == 0, 1 - core, core)
            columns = pl.ds(pl.multiple_of(chunk * head, head), head)
            wg[chunk] = t_dot(xall[:, columns], qkv[...]).astype(BF16)
            return carried

        lax.fori_loop(0, 2, step, 0)
        send(slot("pair", n), wg.at[first + 1 - core], pair1.at[n], partner)

    def add_pair(n):
        chunk = wrap(y + ahead[n]) * 2 + core
        arrived(slot("pair", n), pair1.at[n])
        wg[chunk] = (wg[chunk].astype(F32) + pair1[n].astype(F32)).astype(BF16)

    weight_parts(0)
    for half in range(2):
        take_second(half, 2)
    for half in range(2):
        for side in SIDES:
            rows = sum_rows(sum_block(half, 0, 2), part_start(half, side), PART)
            send(slot("G1", half, side), part.at[rows, :], second1.at[half, which(side)], g_device(half, side))
    for half in range(2):
        send_second(half, 0)

    weight_parts(1)
    weight_parts(2)
    add_pair(0)
    for side in SIDES:
        chunk = wrap(y + 2) * 2 + core
        rows = pl.ds(0 if side == 1 else BLOCK, BLOCK)
        send(slot("Y1", side), wg.at[chunk, rows, :], ring1.at[which(side)], along_y(side))
    add_pair(1)
    weight_parts(3)
    add_pair(2)
    for side in SIDES:
        chunk = wrap(y + side) * 2 + core
        rows = pl.ds(0 if side == 1 else BLOCK, BLOCK)
        arrived(slot("Y1", side), ring1.at[which(side)])
        wg[chunk, rows, :] = (wg[chunk, rows, :].astype(F32) + ring1[which(side)].astype(F32)).astype(BF16)
        send(slot("Y2", side), wg.at[chunk], ring2.at[which(side)], along_y(side))
    add_pair(3)

    for j in (1, 3):
        for half in range(2):
            take_second(half, j)
    for half in range(2):
        for side in SIDES:
            block = sum_block(half, 0, side)
            arrived(slot("G1", half, side), second1.at[half, which(side)])
            add_into(part, sum_rows(block, part_start(half, side), PART), [second1[half, which(side)]])
            rows = sum_rows(block, half * HALF, HALF)
            send(slot("G2", half, side), part.at[rows, :], second2.at[half, which(side)], g_device(half, side))

    for half in range(2):
        take_second(half, 0)

    for side in SIDES:
        arrived(slot("Y2", side), ring2.at[which(side)])
    done_w[...] = wg[y * 2 + core].astype(F32) + ring2[0].astype(F32) + ring2[1].astype(F32)
    leave_w = pltpu.make_async_copy(done_w, out_w, local_sem.at[6])
    leave_w.start()

    for half in range(2):
        for side in SIDES:
            arrived(slot("G2", half, side), second2.at[half, which(side)])
        rows = sum_rows(sp, half * HALF, HALF)
        total = part[rows, :].astype(F32) + second2[half, 0].astype(F32) + second2[half, 1].astype(F32)
        done_x[half * HALF : (half + 1) * HALF, :] = total.astype(BF16)
    leave_x = pltpu.make_async_copy(done_x, out_x.at[0], local_sem.at[7])
    leave_x.start()
    leave_w.wait()
    leave_x.wait()

    for half in range(2):
        for side in SIDES:
            for j in range(RING):
                source = first1.at[half, which(side), j]
                copy(firsts[half, side] + j, source, source, partner).wait_send()
    for index, source in sent:
        copy(index, source, source, partner).wait_send()


A2A_ORDER = (1, 15, 4, 12, 3, 5, 11, 13, 2, 14, 8, 6, 7, 9, 10)
COPIES = 160
LATER = 0
VMEM_LIMIT = 67043328


def split_kernel(sum_x, sum_w, out_x, out_q, out_k, out_v, held_x, held_w, thirds, sems):
    head = out_q.shape[1]
    load_w = pltpu.make_async_copy(sum_w, held_w, sems.at[0])
    load_x = pltpu.make_async_copy(sum_x, held_x, sems.at[1])
    load_w.start()
    load_x.start()
    load_x.wait()
    leave_x = pltpu.make_async_copy(held_x, out_x, sems.at[2])
    leave_x.start()
    load_w.wait()
    leaves = [leave_x]
    for place, out in enumerate((out_q, out_k, out_v)):
        thirds[place] = held_w[:, place * head : (place + 1) * head] * (1.0 / (2 * RING))
        leave = pltpu.make_async_copy(thirds.at[place], out, sems.at[3 + place])
        leave.start()
        leaves.append(leave)
    for leave in leaves:
        leave.wait()


def body(hidden_in, mix_cotangent, query_weight, key_weight, value_weight, decay_log):
    depth = hidden_in.shape[2]
    head = query_weight.shape[1]
    blocks = RING * RING
    length = blocks * BLOCK
    wide = 3 * head
    anywhere = pl.BlockSpec(memory_space=pl.ANY)
    sum_x, sum_w = pl.pallas_call(
        all_kernel,
        out_shape=(
            jax.ShapeDtypeStruct(hidden_in.shape, BF16),
            jax.ShapeDtypeStruct((head, wide), F32),
        ),
        in_specs=[pl.BlockSpec(memory_space=pltpu.HBM)] + [anywhere] * 5,
        out_specs=(anywhere,) * 2,
        scratch_shapes=[
            pltpu.VMEM((length, depth), BF16),
            pltpu.VMEM((depth, wide), BF16),
            pltpu.VMEM((length, wide), BF16),
            pltpu.VMEM((length, head), BF16),
            pltpu.VMEM((length, wide), F32),
            pltpu.VMEM((BLOCK, BLOCK), F32),
            pltpu.VMEM((BLOCK, BLOCK), F32),
            pltpu.VMEM((BLOCK, head), F32),
            pltpu.VMEM((BLOCK, head), F32),
            pltpu.VMEM((blocks, head, head), F32),
            pltpu.VMEM((blocks, head, head), F32),
            pltpu.VMEM((blocks, head, head), BF16),
            pltpu.VMEM((blocks, head, head), BF16),
            pltpu.VMEM((length, depth), BF16),
            pltpu.VMEM((2, 2, RING, PART, depth), BF16),
            pltpu.VMEM((2, 2, RING, HALF, depth), BF16),
            pltpu.VMEM((2, 2, PART, depth), BF16),
            pltpu.VMEM((2, 2, HALF, depth), BF16),
            pltpu.VMEM((2 * RING, depth // (2 * RING), wide), BF16),
            pltpu.VMEM((RING, depth // (2 * RING), wide), BF16),
            pltpu.VMEM((2, depth // (4 * RING), wide), BF16),
            pltpu.VMEM((2, depth // (2 * RING), wide), BF16),
            pltpu.SemaphoreType.DMA((8,)),
            pltpu.SemaphoreType.DMA((COPIES,)),
            pltpu.SemaphoreType.DMA((COPIES,)),
            pltpu.SemaphoreType.REGULAR((4,)),
            pltpu.SMEM((1,), F32),
            pltpu.VMEM((BLOCK, depth), BF16),
            pltpu.VMEM((head, wide), F32),
            pltpu.VMEM((wide, depth), BF16),
        ],
        compiler_params=pltpu.CompilerParams(
            vmem_limit_bytes=VMEM_LIMIT, collective_id=0, has_side_effects=True
        ),
        cost_estimate=pl.CostEstimate(flops=21 * 10**9, bytes_accessed=4 * 10**6, transcendentals=0),
    )(decay_log, hidden_in, mix_cotangent, query_weight, key_weight, value_weight)
    return pl.pallas_call(
        split_kernel,
        out_shape=(
            jax.ShapeDtypeStruct(hidden_in.shape, BF16),
            jax.ShapeDtypeStruct((head, head), F32),
            jax.ShapeDtypeStruct((head, head), F32),
            jax.ShapeDtypeStruct((head, head), F32),
        ),
        in_specs=[anywhere] * 2,
        out_specs=(anywhere,) * 4,
        scratch_shapes=[
            pltpu.VMEM(hidden_in.shape, BF16),
            pltpu.VMEM((head, wide), F32),
            pltpu.VMEM((3, head, head), F32),
            pltpu.SemaphoreType.DMA((6,)),
        ],
    )(sum_x, sum_w)


def solution(mesh):
    placed = (P("dp", "sp", None), P("dp", "sp", None), P("dp", "sp"), P("dp", "sp"), P("dp", "sp"), P("sp"))
    return jax.shard_map(
        body,
        mesh=mesh,
        in_specs=placed,
        out_specs=(P("dp", "sp", None), P("dp", "sp"), P("dp", "sp"), P("dp", "sp")),
        check_vma=False,
    )
```

```python
import jax
import jax.numpy as jnp
from jax import lax
from jax.experimental import pallas as pl
from jax.experimental.pallas import tpu as pltpu
from jax.sharding import PartitionSpec as P

BLOCK = 128
HALF = 64
PART = 32
RING = 4
F32 = jnp.float32
BF16 = jnp.bfloat16
MESH = pl.DeviceIdType.MESH
SIDES = (1, -1)


def dot(a, b):
    return lax.dot_general(a, b, (((1,), (0,)), ((), ())), preferred_element_type=F32)


def dot_t(a, b):
    return lax.dot_general(a, b, (((1,), (1,)), ((), ())), preferred_element_type=F32)


def t_dot(a, b):
    return lax.dot_general(a, b, (((0,), (0,)), ((), ())), preferred_element_type=F32)


def rows_of(block):
    return pl.ds(pl.multiple_of(block * BLOCK, BLOCK), BLOCK)


def pick(index, values):
    got = jnp.int32(values[-1])
    for place, value in enumerate(values[:-1]):
        got = jnp.where(index == place, jnp.int32(value), got)
    return got


def add_into(target, rows, others):
    total = target[rows, :].astype(F32)
    for other in others:
        total = total + other.astype(F32)
    target[rows, :] = total.astype(BF16)


def make_decays(rate, inner_ref, inner_t_ref, query_ref, key_ref):
    row = lax.broadcasted_iota(jnp.int32, (BLOCK, BLOCK), 0)
    col = lax.broadcasted_iota(jnp.int32, (BLOCK, BLOCK), 1)
    spread = (row - col).astype(F32)
    inner_ref[...] = jnp.where(spread >= 0, jnp.exp(rate * jnp.maximum(spread, 0.0)), 0.0)
    inner_t_ref[...] = jnp.where(spread <= 0, jnp.exp(rate * jnp.maximum(-spread, 0.0)), 0.0)
    offset = lax.broadcasted_iota(jnp.int32, query_ref.shape, 0).astype(F32)
    query_ref[...] = jnp.exp(rate * (offset + 1.0))
    key_ref[...] = jnp.exp(rate * (BLOCK - 1.0 - offset))


def in_block(block, head, scale, qkv, cot, decays, grads, fwd_states, bwd_states):
    inner_ref, inner_t_ref, query_ref, key_ref = decays
    rows = rows_of(block)
    queries = qkv[rows, 0:head]
    keys = qkv[rows, head : 2 * head]
    values = qkv[rows, 2 * head : 3 * head]
    given = cot[rows, :]
    mixed = (dot_t(given, values) * inner_ref[...]).astype(BF16)
    grads[rows, 0:head] = dot(mixed, keys)
    mixed_t = (dot_t(values, given) * inner_t_ref[...]).astype(BF16)
    grads[rows, head : 2 * head] = dot(mixed_t, queries) * scale
    scores_t = (dot_t(keys, queries) * inner_t_ref[...]).astype(BF16)
    grads[rows, 2 * head : 3 * head] = dot(scores_t, given)
    keys_w = (keys.astype(F32) * key_ref[...]).astype(BF16)
    fwd_states[block] = t_dot(keys_w, values)
    queries_w = (queries.astype(F32) * query_ref[...]).astype(BF16)
    bwd_states[block] = t_dot(queries_w, given)


def run_states(rate, blocks, fwd_states, bwd_states, fwd_bf, bwd_bf):
    size = 32
    wide = fwd_states.shape[2]
    step = jnp.exp(jnp.full((size, wide), BLOCK, F32) * rate)

    def chunk(n, carried):
        rows = pl.ds(pl.multiple_of(n * size, size), size)
        ahead = jnp.zeros((size, wide), F32)
        back = jnp.zeros((size, wide), F32)
        for i in range(blocks):
            fwd_bf[i, rows, :] = ahead.astype(BF16)
            ahead = ahead * step + fwd_states[i, rows, :]
            last = blocks - 1 - i
            bwd_bf[last, rows, :] = back.astype(BF16)
            back = back * step + bwd_states[last, rows, :]
        return carried

    lax.fori_loop(0, fwd_states.shape[1] // size, chunk, 0)


def cross_block(block, head, scale, qkv, cot, decays, grads, fwd_bf, bwd_bf, out):
    _, _, query_ref, key_ref = decays
    rows = rows_of(block)
    keys = qkv[rows, head : 2 * head]
    values = qkv[rows, 2 * head : 3 * head]
    state = fwd_bf[block]
    back = bwd_bf[block]
    grad_q = grads[rows, 0:head] + dot_t(cot[rows, :], state) * query_ref[...]
    grad_k = grads[rows, head : 2 * head] + dot_t(values, back) * (key_ref[...] * scale)
    grad_v = grads[rows, 2 * head : 3 * head] + dot(keys, back) * key_ref[...]
    out[rows, 0:head] = grad_q.astype(BF16)
    out[rows, head : 2 * head] = grad_k.astype(BF16)
    out[rows, 2 * head : 3 * head] = grad_v.astype(BF16)


def all_kernel(
    rate_ref,
    own_x,
    own_cot,
    wq_ref,
    wk_ref,
    wv_ref,
    out_x,
    out_w,
    xall,
    w,
    qkv,
    cot,
    grads,
    inner,
    inner_t,
    query_d,
    key_d,
    fwd,
    bwd,
    fwd_bf,
    bwd_bf,
    part,
    first1,
    first2,
    second1,
    second2,
    wg,
    pair1,
    ring1,
    ring2,
    local_sem,
    send_sem,
    recv_sem,
    ready_sem,
    rate_smem,
    done_x,
    done_w,
    wt,
):
    depth = xall.shape[1]
    head = cot.shape[1]
    blocks = RING * RING
    scale = head ** (-0.5)
    sp = lax.axis_index("sp")
    dp = lax.axis_index("dp")
    z, x = lax.div(sp, RING), lax.rem(sp, RING)
    y, core = lax.div(dp, 2), lax.rem(dp, 2)
    decays = (inner, inner_t, query_d, key_d)
    names = {}
    sent = []

    def slot(*name):
        return names.setdefault(name, len(names))

    def slots(count, *name):
        first = slot(*name, 0)
        for place in range(1, count):
            assert slot(*name, place) == first + place
        return first

    def wrap(value):
        return lax.rem(value + RING, RING)

    def block_at(dz, dx):
        return wrap(z + dz) * RING + wrap(x + dx)

    def plane(dz, dx):
        return (block_at(dz, dx), dp)

    def along_y(dy):
        return (sp, wrap(y + dy) * 2 + core)

    partner = (sp, y * 2 + 1 - core)

    def along(half, first, second):
        return (second, first) if half == 0 else (first, second)

    def copy(index, source, target, device):
        return pltpu.make_async_remote_copy(
            src_ref=source,
            dst_ref=target,
            send_sem=send_sem.at[index],
            recv_sem=recv_sem.at[index],
            device_id=device,
            device_id_type=MESH,
        )

    def send(index, source, target, device):
        copy(index, source, target, device).start()
        sent.append((index, source))

    def send_in_loop(index, source, target, device):
        copy(index, source, target, device).start()

    def arrived(index, target):
        copy(index, target, target, partner).wait_recv()

    barrier = pltpu.get_barrier_semaphore()
    beside = [plane(0, 1), plane(0, -1), plane(1, 0), plane(-1, 0)]
    friends = beside + [along_y(1), along_y(-1), partner]
    for friend in friends:
        pl.semaphore_signal(barrier, inc=1, device_id=friend, device_id_type=MESH)

    own_rows = rows_of(sp)
    w_rows = pl.ds(pl.multiple_of(dp * head, head), head)
    loads = [
        pltpu.make_async_copy(own_x.at[0], xall.at[own_rows, :], local_sem.at[0]),
        pltpu.make_async_copy(wq_ref, w.at[w_rows, 0:head], local_sem.at[1]),
        pltpu.make_async_copy(wk_ref, w.at[w_rows, head : 2 * head], local_sem.at[2]),
        pltpu.make_async_copy(wv_ref, w.at[w_rows, 2 * head : 3 * head], local_sem.at[3]),
        pltpu.make_async_copy(
            own_cot.at[0, :, pl.ds(pl.multiple_of(sp * head, head), head)], cot.at[own_rows, :], local_sem.at[4]
        ),
    ]
    loads.append(pltpu.make_async_copy(rate_ref, rate_smem, local_sem.at[5]))
    for load in loads:
        load.start()
    for load in loads:
        load.wait()
    rate = rate_smem[0]
    pl.semaphore_wait(barrier, len(friends))

    def x_rows(block, start, count):
        return xall.at[pl.ds(pl.multiple_of(block * BLOCK + start, PART), count), :]

    def part_start(half, side):
        return half * HALF + (0 if side == 1 else PART)

    def gather_block(half, p, q):
        return block_at(*along(half, p, q))

    def gather_send(name, half, p, q, side, axis):
        block = gather_block(half, p, q)
        if name[0] in ("s1", "s2"):
            rows = x_rows(block, half * HALF, HALF)
        else:
            rows = x_rows(block, part_start(half, side), PART)
        device = plane(*along(half, side, 0)) if axis == 0 else plane(*along(half, 0, side))
        send(slot(*name), rows, rows, device)

    def gather_wait(name, half, p, q, side):
        block = gather_block(half, p, q)
        if name[0] in ("s1", "s2"):
            rows = x_rows(block, half * HALF, HALF)
        else:
            rows = x_rows(block, part_start(half, side), PART)
        arrived(slot(*name), rows)

    def w_part(dy, which, start, count):
        first = (wrap(y + dy) * 2 + which) * head
        return w.at[pl.ds(pl.multiple_of(first + start, BLOCK), count), :]

    for side in SIDES:
        send(slot("w1", side), w_part(0, core, 0, head), w_part(0, core, 0, head), along_y(side))
    send(slot("wc", 0), w_part(0, core, 0, head), w_part(0, core, 0, head), partner)

    def exchange():
        for turn in range(3):
            for friend in beside:
                pl.semaphore_signal(ready_sem.at[turn], inc=1, device_id=friend, device_id_type=MESH)
            pl.semaphore_wait(ready_sem.at[turn], len(beside))
        for offset in A2A_ORDER:
            target = lax.rem(sp + offset, blocks)
            send_in_loop(
                slot("cot", offset),
                own_cot.at[0, :, pl.ds(pl.multiple_of(target * head, head), head)],
                cot.at[own_rows, :],
                (target, dp),
            )

    for offset in A2A_ORDER:
        sent.append((slot("cot", offset), cot.at[0:BLOCK, :]))

    @pl.when(core == LATER)
    def _():
        exchange()
        pl.semaphore_wait(ready_sem.at[3], 1)

    for half in range(2):
        for side in SIDES:
            gather_send(("s1", half, side), half, 0, 0, side, 0)
    for half in range(2):
        for side in SIDES:
            gather_send(("s2", half, 0, side), half, 0, 0, side, 1)
    pl.when(core != LATER)(exchange)
    make_decays(rate, *decays)

    def project(block):
        rows = rows_of(block)
        got = dot(xall[rows, :], w[...])
        qkv[rows, 0:head] = got[:, 0:head].astype(BF16)
        qkv[rows, head : 2 * head] = (got[:, head : 2 * head].astype(BF16).astype(F32) * scale).astype(BF16)
        qkv[rows, 2 * head : 3 * head] = got[:, 2 * head : 3 * head].astype(BF16)

    def inside(block):
        in_block(block, head, scale, qkv, cot, decays, grads, fwd, bwd)

    def loop(places, *works):
        several = 2 if len(places) % 2 == 0 else 1

        def step(n, carried):
            group = []
            for m in range(several):
                at = n * several + m
                group.append(block_at(pick(at, [dz for dz, _ in places]), pick(at, [dx for _, dx in places])))
            for work in works:
                for block in group:
                    work(block)
            return carried

        lax.fori_loop(0, len(places) // several, step, 0)

    near = [(0, 0), (0, 1), (0, 3), (1, 0), (3, 0)]
    corners = [(1, 1), (1, 3), (3, 1), (3, 3)]
    far = [(0, 2), (2, 0)]
    last = [(2, 2)]

    for half in range(2):
        for side in SIDES:
            gather_wait(("s1", half, side), half, -side, 0, side)
            gather_send(("f1", half, side), half, -side, 0, side, 0)
    for half in range(2):
        for near_p in SIDES:
            for side in SIDES:
                gather_send(("s2", half, near_p, side), half, near_p, 0, side, 1)

    for side in SIDES:
        arrived(slot("w1", side), w_part(-side, core, 0, head))
        rows = w_part(-side, core, 0 if side == 1 else BLOCK, BLOCK)
        send(slot("w2", side), rows, rows, along_y(side))
        rows = w_part(-side, core, 0, head)
        send(slot("wc", side), rows, rows, partner)

    @pl.when(core != LATER)
    def _():
        pl.semaphore_signal(ready_sem.at[3], inc=1, device_id=partner, device_id_type=MESH)

    for half in range(2):
        for side in SIDES:
            gather_wait(("s2", half, 0, side), half, 0, -side, side)
            gather_send(("f2", half, 0, side), half, 0, -side, side, 1)

    for side in SIDES:
        arrived(slot("w2", side), w_part(2, core, 0 if side == 1 else BLOCK, BLOCK))
    send(slot("wc", 2), w_part(2, core, 0, head), w_part(2, core, 0, head), partner)
    for dy in (0, 1, -1, 2):
        arrived(slot("wc", dy), w_part(-dy, 1 - core, 0, head))

    loop(near, project)

    def turn_weights(n, carried):
        rows = pl.ds(pl.multiple_of(n * head, head), head)
        for third in range(3):
            wt[third * head : (third + 1) * head, rows] = w[rows, third * head : (third + 1) * head].T
        return carried

    lax.fori_loop(0, depth // head, turn_weights, 0)

    for half in range(2):
        for side in SIDES:
            gather_wait(("f1", half, side), half, 2, 0, side)
    for half in range(2):
        for side in SIDES:
            gather_send(("s2", half, 2, side), half, 2, 0, side, 1)

    for offset in A2A_ORDER:
        arrived(slot("cot", offset), cot.at[rows_of(lax.rem(sp + blocks - offset, blocks)), :])
    loop(near, inside)

    for near_p in SIDES:
        for half in range(2):
            for side in SIDES:
                gather_wait(("s2", half, near_p, side), half, near_p, -side, side)
                gather_send(("f2", half, near_p, side), half, near_p, -side, side, 1)
    loop(corners, project, inside)

    for half in range(2):
        for side in SIDES:
            gather_wait(("f2", half, 0, side), half, 0, 2, side)
    loop(far, project, inside)

    for half in range(2):
        for side in SIDES:
            gather_wait(("s2", half, 2, side), half, 2, -side, side)
            gather_send(("f2", half, 2, side), half, 2, -side, side, 1)

    for near_p in SIDES:
        for half in range(2):
            for side in SIDES:
                gather_wait(("f2", half, near_p, side), half, near_p, 2, side)
        loop([(2, near_p), (near_p, 2)], project, inside)

    for half in range(2):
        for side in SIDES:
            gather_wait(("f2", half, 2, side), half, 2, 2, side)
    loop(last, project, inside)

    run_states(rate, blocks, fwd, bwd, fwd_bf, bwd_bf)

    def finish_all(group):
        for block in group:
            cross_block(block, head, scale, qkv, cot, decays, grads, fwd_bf, bwd_bf, qkv)
        got = jnp.concatenate([qkv[rows_of(block), :] for block in group], axis=0)
        sums = dot(got, wt[...]).astype(BF16)
        for place, block in enumerate(group):
            part[rows_of(block), :] = sums[place * BLOCK : (place + 1) * BLOCK, :]

    def finish_loop(places):
        def step(n, carried):
            group = []
            for m in range(2):
                at = n * 2 + m
                group.append(block_at(pick(at, [dz for dz, _ in places]), pick(at, [dx for _, dx in places])))
            finish_all(group)
            return carried

        lax.fori_loop(0, len(places) // 2, step, 0)

    def sum_block(half, f, q):
        return block_at(*((f, q) if half == 0 else (q, f)))

    def sum_rows(block, start, count):
        return pl.ds(pl.multiple_of(block * BLOCK + start, PART), count)

    def f_device(half, side):
        return plane(side, 0) if half == 0 else plane(0, side)

    def g_device(half, side):
        return plane(0, side) if half == 0 else plane(side, 0)

    def which(side):
        return 0 if side == 1 else 1

    firsts = {(half, side): slots(RING, "F1", half, side) for half in range(2) for side in SIDES}

    def send_first(half, j):
        for side in SIDES:
            rows = sum_rows(sum_block(half, 2, j), part_start(half, side), PART)
            send_in_loop(
                firsts[half, side] + j, part.at[rows, :], first1.at[half, which(side), j], f_device(half, side)
            )

    def send_second(half, j):
        for side in SIDES:
            block = sum_block(half, side, j)
            rows = sum_rows(block, part_start(half, side), PART)
            arrived(firsts[half, side] + j, first1.at[half, which(side), j])
            add_into(part, rows, [first1[half, which(side), j]])
        for side in SIDES:
            block = sum_block(half, side, j)
            rows = sum_rows(block, half * HALF, HALF)
            send(slot("F2", half, j, side), part.at[rows, :], first2.at[half, which(side), j], f_device(half, side))

    def take_second(half, j):
        for side in SIDES:
            arrived(slot("F2", half, j, side), first2.at[half, which(side), j])
        rows = sum_rows(sum_block(half, 0, j), half * HALF, HALF)
        add_into(part, rows, [first2[half, 0, j], first2[half, 1, j]])

    finish_all([block_at(2, 2)])
    for half in range(2):
        send_first(half, 2)

    def outer(n, carried):
        place = pick(n, (1, 3, 0))
        finish_all([block_at(2, place), block_at(place, 2)])
        for half in range(2):
            send_first(half, place)
        return carried

    lax.fori_loop(0, 3, outer, 0)
    for half in range(2):
        send_second(half, 2)
    finish_loop(corners)
    for j in (1, 3):
        for half in range(2):
            send_second(half, j)
    finish_loop([(1, 0), (3, 0), (0, 1), (0, 3)])
    finish_all([block_at(0, 0)])

    ahead = (2, 1, 3, 0)

    def weight_parts(n):
        first = wrap(y + ahead[n]) * 2

        def step(i, carried):
            chunk = first + jnp.where(i == 0, 1 - core, core)
            columns = pl.ds(pl.multiple_of(chunk * head, head), head)
            wg[chunk] = t_dot(xall[:, columns], qkv[...]).astype(BF16)
            return carried

        lax.fori_loop(0, 2, step, 0)
        send(slot("pair", n), wg.at[first + 1 - core], pair1.at[n], partner)

    def add_pair(n):
        chunk = wrap(y + ahead[n]) * 2 + core
        arrived(slot("pair", n), pair1.at[n])
        wg[chunk] = (wg[chunk].astype(F32) + pair1[n].astype(F32)).astype(BF16)

    weight_parts(0)
    for half in range(2):
        take_second(half, 2)
    for half in range(2):
        for side in SIDES:
            rows = sum_rows(sum_block(half, 0, 2), part_start(half, side), PART)
            send(slot("G1", half, side), part.at[rows, :], second1.at[half, which(side)], g_device(half, side))
    for half in range(2):
        send_second(half, 0)

    weight_parts(1)
    weight_parts(2)
    add_pair(0)
    for side in SIDES:
        chunk = wrap(y + 2) * 2 + core
        rows = pl.ds(0 if side == 1 else BLOCK, BLOCK)
        send(slot("Y1", side), wg.at[chunk, rows, :], ring1.at[which(side)], along_y(side))
    add_pair(1)
    weight_parts(3)
    add_pair(2)
    for side in SIDES:
        chunk = wrap(y + side) * 2 + core
        rows = pl.ds(0 if side == 1 else BLOCK, BLOCK)
        arrived(slot("Y1", side), ring1.at[which(side)])
        wg[chunk, rows, :] = (wg[chunk, rows, :].astype(F32) + ring1[which(side)].astype(F32)).astype(BF16)
        send(slot("Y2", side), wg.at[chunk], ring2.at[which(side)], along_y(side))
    add_pair(3)

    for j in (1, 3):
        for half in range(2):
            take_second(half, j)
    for half in range(2):
        for side in SIDES:
            block = sum_block(half, 0, side)
            arrived(slot("G1", half, side), second1.at[half, which(side)])
            add_into(part, sum_rows(block, part_start(half, side), PART), [second1[half, which(side)]])
            rows = sum_rows(block, half * HALF, HALF)
            send(slot("G2", half, side), part.at[rows, :], second2.at[half, which(side)], g_device(half, side))

    for half in range(2):
        take_second(half, 0)

    for side in SIDES:
        arrived(slot("Y2", side), ring2.at[which(side)])
    done_w[...] = wg[y * 2 + core].astype(F32) + ring2[0].astype(F32) + ring2[1].astype(F32)
    leave_w = pltpu.make_async_copy(done_w, out_w, local_sem.at[6])
    leave_w.start()

    for half in range(2):
        for side in SIDES:
            arrived(slot("G2", half, side), second2.at[half, which(side)])
        rows = sum_rows(sp, half * HALF, HALF)
        total = part[rows, :].astype(F32) + second2[half, 0].astype(F32) + second2[half, 1].astype(F32)
        done_x[half * HALF : (half + 1) * HALF, :] = total.astype(BF16)
    leave_x = pltpu.make_async_copy(done_x, out_x.at[0], local_sem.at[7])
    leave_x.start()
    leave_w.wait()
    leave_x.wait()

    for half in range(2):
        for side in SIDES:
            for j in range(RING):
                source = first1.at[half, which(side), j]
                copy(firsts[half, side] + j, source, source, partner).wait_send()
    for index, source in sent:
        copy(index, source, source, partner).wait_send()


A2A_ORDER = (1, 15, 4, 12, 3, 5, 11, 13, 2, 14, 8, 6, 7, 9, 10)
COPIES = 160
LATER = 0
VMEM_LIMIT = 67043328


def split_kernel(sum_x, sum_w, out_x, out_q, out_k, out_v, held_x, held_w, thirds, sems):
    head = out_q.shape[1]
    load_w = pltpu.make_async_copy(sum_w, held_w, sems.at[0])
    load_x = pltpu.make_async_copy(sum_x, held_x, sems.at[1])
    load_w.start()
    load_x.start()
    load_x.wait()
    leave_x = pltpu.make_async_copy(held_x, out_x, sems.at[2])
    leave_x.start()
    load_w.wait()
    leaves = [leave_x]
    for place, out in enumerate((out_q, out_k, out_v)):
        thirds[place] = held_w[:, place * head : (place + 1) * head] * (1.0 / (2 * RING))
        leave = pltpu.make_async_copy(thirds.at[place], out, sems.at[3 + place])
        leave.start()
        leaves.append(leave)
    for leave in leaves:
        leave.wait()


def body(hidden_in, mix_cotangent, query_weight, key_weight, value_weight, decay_log):
    depth = hidden_in.shape[2]
    head = query_weight.shape[1]
    blocks = RING * RING
    length = blocks * BLOCK
    wide = 3 * head
    anywhere = pl.BlockSpec(memory_space=pl.ANY)
    sum_x, sum_w = pl.pallas_call(
        all_kernel,
        out_shape=(
            jax.ShapeDtypeStruct(hidden_in.shape, BF16),
            jax.ShapeDtypeStruct((head, wide), F32),
        ),
        in_specs=[pl.BlockSpec(memory_space=pltpu.HBM)] + [anywhere] * 5,
        out_specs=(anywhere,) * 2,
        scratch_shapes=[
            pltpu.VMEM((length, depth), BF16),
            pltpu.VMEM((depth, wide), BF16),
            pltpu.VMEM((length, wide), BF16),
            pltpu.VMEM((length, head), BF16),
            pltpu.VMEM((length, wide), F32),
            pltpu.VMEM((BLOCK, BLOCK), F32),
            pltpu.VMEM((BLOCK, BLOCK), F32),
            pltpu.VMEM((BLOCK, head), F32),
            pltpu.VMEM((BLOCK, head), F32),
            pltpu.VMEM((blocks, head, head), F32),
            pltpu.VMEM((blocks, head, head), F32),
            pltpu.VMEM((blocks, head, head), BF16),
            pltpu.VMEM((blocks, head, head), BF16),
            pltpu.VMEM((length, depth), BF16),
            pltpu.VMEM((2, 2, RING, PART, depth), BF16),
            pltpu.VMEM((2, 2, RING, HALF, depth), BF16),
            pltpu.VMEM((2, 2, PART, depth), BF16),
            pltpu.VMEM((2, 2, HALF, depth), BF16),
            pltpu.VMEM((2 * RING, depth // (2 * RING), wide), BF16),
            pltpu.VMEM((RING, depth // (2 * RING), wide), BF16),
            pltpu.VMEM((2, depth // (4 * RING), wide), BF16),
            pltpu.VMEM((2, depth // (2 * RING), wide), BF16),
            pltpu.SemaphoreType.DMA((8,)),
            pltpu.SemaphoreType.DMA((COPIES,)),
            pltpu.SemaphoreType.DMA((COPIES,)),
            pltpu.SemaphoreType.REGULAR((4,)),
            pltpu.SMEM((1,), F32),
            pltpu.VMEM((BLOCK, depth), BF16),
            pltpu.VMEM((head, wide), F32),
            pltpu.VMEM((wide, depth), BF16),
        ],
        compiler_params=pltpu.CompilerParams(
            vmem_limit_bytes=VMEM_LIMIT, collective_id=0, has_side_effects=True
        ),
        cost_estimate=pl.CostEstimate(flops=21 * 10**9, bytes_accessed=4 * 10**6, transcendentals=0),
    )(decay_log, hidden_in, mix_cotangent, query_weight, key_weight, value_weight)
    return pl.pallas_call(
        split_kernel,
        out_shape=(
            jax.ShapeDtypeStruct(hidden_in.shape, BF16),
            jax.ShapeDtypeStruct((head, head), F32),
            jax.ShapeDtypeStruct((head, head), F32),
            jax.ShapeDtypeStruct((head, head), F32),
        ),
        in_specs=[anywhere] * 2,
        out_specs=(anywhere,) * 4,
        scratch_shapes=[
            pltpu.VMEM(hidden_in.shape, BF16),
            pltpu.VMEM((head, wide), F32),
            pltpu.VMEM((3, head, head), F32),
            pltpu.SemaphoreType.DMA((6,)),
        ],
    )(sum_x, sum_w)


def solution(mesh):
    placed = (P("dp", "sp", None), P("dp", "sp", None), P("dp", "sp"), P("dp", "sp"), P("dp", "sp"), P("sp"))
    return jax.shard_map(
        body,
        mesh=mesh,
        in_specs=placed,
        out_specs=(P("dp", "sp", None), P("dp", "sp"), P("dp", "sp"), P("dp", "sp")),
        check_vma=False,
    )
```
